32 devices in a mesh: sp: 4 (over y, x), tp: 8 (over z, core).
Axes of the slice: x: 2, y: 2, z: 4, core: 2. Of those that a mesh axis runs over, the one named last changes fastest.
Arguments:
- moe_input: bfloat16 [512, 2048], P('sp'), may hold values from -6 to 6
- cotangent: bfloat16 [512, 2048], P('sp'), may hold values from -6 to 6
- route_expert: int32 [512, 2], P('sp'), may hold values from 0 to 3, all different within a row; in each aligned block of 128 rows (0 to 127, 128 to 255, ...) at most 128 rows name the same one
- route_weight: float32 [512, 2], P('sp'), may hold values from 0.2 to 1
- w_gate: bfloat16 [4, 2048, 6144], P('sp', None, 'tp'), may hold values from -0.125 to 0.125
- w_up: bfloat16 [4, 2048, 6144], P('sp', None, 'tp'), may hold values from -0.125 to 0.125
- w_down: bfloat16 [4, 6144, 2048], P('sp', 'tp'), may hold values from -0.078125 to 0.078125
- out_proj: bfloat16 [2048, 2048], P('tp'), may hold values from -0.125 to 0.125
- saved_out: bfloat16 [512, 2048], P('sp', 'tp'), may hold values from -6 to 6
- queries: bfloat16 [512, 1024], P('sp', 'tp'), may hold values from -6 to 6
- keys: bfloat16 [512, 1024], P('sp', 'tp'), may hold values from -6 to 6
- values: bfloat16 [512, 2048], P('sp', 'tp'), may hold values from -6 to 6
- log_decay: float32 [512, 1024], P('sp', 'tp'), may hold values from -1 to 0
- span_state: float32 [8, 1024, 128], P('sp', 'tp'), may hold values from -6 to 6
Outputs:
- grad_w_gate: bfloat16 [4, 2048, 6144], P('sp', None, 'tp')
- grad_w_up: bfloat16 [4, 2048, 6144], P('sp', None, 'tp')
- grad_w_down: bfloat16 [4, 6144, 2048], P('sp', 'tp')
- grad_proj: float32 [2048, 2048], P('sp', 'tp')
- grad_queries: bfloat16 [512, 1024], P('sp', 'tp')
- grad_keys: bfloat16 [512, 1024], P('sp', 'tp')
- grad_values: bfloat16 [512, 2048], P('sp', 'tp')
- grad_decay: float32 [512, 1024], P('sp', 'tp')
The draws below stay inside these ranges and needn't reach their ends.
Inputs may be any that keep to these rules, and one draw needn't show every extreme that they name: `route_expert`: each row names two different experts. Within the 128 rows of one index of sp no expert is named by more than 128 rows, a bound that some block reaches.
All inputs are finite; a program needn't handle non-finite values.
Results may differ from the reference program's by a relative error of at most 0.019.
Values may be sent and summed in bfloat16 or wider, within the bound.
A program may use at most 128 MiB of HBM per device.

```python
import math
import jax
import jax.numpy as jnp
import numpy as np
from jax import lax

D = 2048
HEADS = 16
DK = 64
DV = 128
F = 6144
SPAN = 64
TOK_DEV = 128
TOKENS = 512
EXPERTS = 4
CAP = 128
N_SP = 4


def draw_log_decay(key, part):
    keys_list = jax.random.split(jax.random.fold_in(key, 11), 7)
    channels = HEADS * DK
    fast_variant = jax.random.uniform(keys_list[0], (channels,)) < 0.5
    slow_rate = jnp.log(10.0) / TOKENS * jax.random.uniform(keys_list[1], (channels,), minval=0.1, maxval=0.4)
    quick_rate = 1.0 / jax.random.uniform(keys_list[2], (channels,), minval=30.0, maxval=50.0)
    starting_offset = jnp.where(fast_variant, quick_rate, slow_rate)
    coarse_estimate = jnp.exp(jax.random.uniform(keys_list[3], (TOKENS, channels), minval=-0.7, maxval=0.7))
    levels = jax.random.uniform(keys_list[4], (TOKENS // TOK_DEV, 1, 1), minval=-0.7, maxval=0.7)
    block_multiplier = jnp.exp(jnp.broadcast_to(levels, (TOKENS // TOK_DEV, TOK_DEV, 1)).reshape(TOKENS, 1))
    target_locations = jax.random.randint(keys_list[5], (3,), 0, TOKENS)
    token_locations = jnp.arange(TOKENS, dtype=jnp.int32)
    transfer_group_rows = jnp.any(token_locations[:, None] == target_locations[None, :], axis=1).astype(jnp.float32)
    layer_stack_depth = -jnp.log(jax.random.uniform(keys_list[6], (channels,), minval=0.5, maxval=0.8))
    transfer_group = transfer_group_rows[:, None] * jnp.where(fast_variant, 0.0, layer_stack_depth)[None, :]
    return (-(starting_offset[None, :] * coarse_estimate * block_multiplier) - transfer_group).astype(jnp.float32)


def raised(values, rng, source, target, shards_of, factor):
    owner, partner = [(jnp.arange(values.shape[position]) // (values.shape[position] // shards_of)).reshape([-1 if axis == position else 1 for axis in range(values.ndim)]) for position in (source, target)]
    chosen = jax.random.permutation(rng, shards_of)[partner]
    strong = (owner == chosen) | (owner == (partner + shards_of // 2) % shards_of)
    return jnp.where(strong, factor * values, values)


def shard_levels(stream_key, dims, cuts, low, top_value):
    gain, own = 1.0, jax.random.fold_in(stream_key, 6)
    for position, blocks in cuts:
        heights = jnp.exp(jax.random.uniform(jax.random.fold_in(own, position), (blocks,), jnp.float32, low / len(cuts), top_value / len(cuts)))
        gain = gain * jnp.repeat(heights, dims[position] // blocks).reshape([-1 if axis == position else 1 for axis in range(len(dims))])
    return gain


def routed_block(own_key, own, number, rows, count, top, limit, slope):
    ranking = jax.random.permutation(own_key, count)
    crowded, ordinary = portions_of(count, rows * top, limit, slope, True), portions_of(count, rows * top, limit, slope, False)
    places = jnp.arange(count)

    def named(lengths, offset_by):
        used = int((lengths > 0).sum())
        fixed = max(1, used // 4)
        moved = fixed + (places - fixed + offset_by * (used - fixed)) % max(1, count - fixed)
        return jnp.zeros((count,), jnp.int32).at[ranking[jnp.where(places < fixed, places, moved)]].set(jnp.asarray(lengths, jnp.int32))

    lengths = jnp.where(number % 4 == 0, named(crowded, number // 4), named(ordinary, number - number // 4 - 1))
    mixed = jax.random.permutation(jax.random.fold_in(own, 3), count)
    source_of, taker = mixed[0:count // 2 * 2:2], mixed[1:count // 2 * 2:2]
    room = jnp.minimum(lengths[source_of] - 1, limit - lengths[taker]) // 2
    room = jnp.where((source_of == ranking[0]) | (taker == ranking[0]) | (lengths[taker] == 0), 0, jnp.maximum(room, 0))
    moved = jax.random.randint(jax.random.fold_in(own, 4), (count // 2,), 0, 1 << 20) % (room + 1)
    lengths = lengths.at[source_of].add(-moved).at[taker].add(moved)
    items = jnp.searchsorted(jnp.cumsum(lengths), jnp.arange(rows * top), side="right").astype(jnp.int32)
    table = items.reshape(top, rows).T
    table = table[jax.random.permutation(jax.random.fold_in(own, 1), rows)]
    offset_by = jax.random.randint(jax.random.fold_in(own, 2), (rows, 1), 0, top)
    return jnp.take_along_axis(table, (jnp.arange(top)[None, :] + offset_by) % top, axis=1)


def portions_of(count, total, bound, lean, full):
    loads = [(1 << 20) // math.isqrt(standing ** lean) + 1 for standing in range(1, count + 1)]
    largest = bound if full else min(bound, max(-(-total // count), total * loads[0] // sum(loads)))
    least = 1 if total - largest >= count - 1 else 0
    holding, spare = [largest] + [least] * (count - 1), total - largest - least * (count - 1)
    while spare > 0:
        free = [i for i in range(1, count) if holding[i] < largest] or [i for i in range(1, count) if holding[i] < bound]
        whole, left = sum([loads[i] for i in free]), spare
        for i in free:
            extra = min(bound - holding[i], max(1, left * loads[i] // whole), spare)
            holding[i] = holding[i] + extra
            spare = spare - extra
    return np.array(holding)


def normal_values(rng, extent, spread, most, shards=(), kind=jnp.bfloat16):
    drawn = spread * jax.random.normal(rng, extent, jnp.float32)
    if shards:
        drawn = drawn * shard_levels(rng, extent, shards, -0.22, 0.18)
    return jnp.clip(drawn, -most, most).astype(kind)


def bell_draw_with(own_key, shape, scale, most, cuts, heavy, held_as=jnp.bfloat16):
    values = scale * jax.random.normal(own_key, shape, jnp.float32)
    if cuts:
        values = values * shard_levels(own_key, shape, cuts, -0.22, 0.18)
    return jnp.clip(raised(values, jax.random.fold_in(own_key, 3), *heavy), -most, most).astype(held_as)


def setup_inputs(seed: int = 0) -> dict:
    seeds = jax.random.split(jax.random.key(seed), 15)
    moe_input = normal_values(seeds[0], (TOKENS, D), 1.0, 6.0, ((0, 4),))
    cotangent = bell_draw_with(seeds[1], (TOKENS, D), 1.0, 6.0, ((0, 4),), (0, 1, 4, 2.0))
    route_expert_keys = jax.random.split(jax.random.fold_in(seeds[2], 1), TOKENS // TOK_DEV)
    route_expert_turns = jax.random.permutation(jax.random.fold_in(seeds[2], 3), TOKENS // TOK_DEV)
    route_expert = jax.vmap(lambda own, number: routed_block(jax.random.fold_in(seeds[2], 2), own, number, TOK_DEV, EXPERTS, 2, CAP, 1))(route_expert_keys, route_expert_turns).reshape((TOKENS, 2))
    route_weight = jnp.clip(0.2 + 0.8 * jax.random.uniform(seeds[3], (TOKENS, 2), jnp.float32) ** shard_levels(seeds[3], (TOKENS, 2), ((0, 4),), -0.2, 0.2), 0.2, 1.0)
    w_gate = normal_values(seeds[4], (EXPERTS, D, F), D ** -0.5, 0.125, ((0, 4), (2, 8)))
    w_up = normal_values(seeds[5], (EXPERTS, D, F), D ** -0.5, 0.125, ((0, 4), (2, 8)))
    w_down = normal_values(seeds[6], (EXPERTS, F, D), F ** -0.5, 0.078125, ((0, 4), (1, 8)))
    out_proj = normal_values(seeds[7], (HEADS * DV, D), (HEADS * DV) ** -0.5, 0.125, ((0, 8),))
    saved_out = normal_values(seeds[8], (TOKENS, HEADS * DV), 1.0, 6.0, ((0, 4), (1, 8)))
    queries = normal_values(seeds[9], (TOKENS, HEADS * DK), 1.0, 6.0, ((0, 4), (1, 8)))
    keys = normal_values(seeds[10], (TOKENS, HEADS * DK), 1.0, 6.0, ((0, 4), (1, 8)))
    values = normal_values(seeds[11], (TOKENS, HEADS * DV), 1.0, 6.0, ((0, 4), (1, 8)))
    log_decay = draw_log_decay(jax.random.fold_in(seeds[14], 71), 0)
    span_state = normal_values(seeds[13], (TOKENS // SPAN, HEADS * DK, DV), 1.0, 6.0, ((0, 4), (1, 8)), jnp.float32)
    return {"moe_input": moe_input, "cotangent": cotangent, "route_expert": route_expert, "route_weight": route_weight, "w_gate": w_gate, "w_up": w_up, "w_down": w_down, "out_proj": out_proj, "saved_out": saved_out, "queries": queries, "keys": keys, "values": values, "log_decay": log_decay, "span_state": span_state}


HIGH = lax.Precision.HIGHEST

def slot_places(experts, count):
    routes_flat = experts.reshape(-1)
    one_hot = (routes_flat[:, None] == jnp.arange(count, dtype=jnp.int32)[None, :]).astype(jnp.int32)
    earlier = jnp.cumsum(one_hot, axis=0) - one_hot
    return lax.optimization_barrier(jnp.sum(earlier * one_hot, axis=1)).reshape(experts.shape).astype(jnp.int32)

def expert_grads(inputs, routed, gate_weight, up_weight, down_weight):
    gate = jnp.dot(inputs, gate_weight, preferred_element_type=jnp.float32)
    upper = jnp.dot(inputs, up_weight, preferred_element_type=jnp.float32)
    sigmoid_gate = jax.nn.sigmoid(gate)
    active = gate * sigmoid_gate
    hidden = (active * upper).astype(jnp.bfloat16)
    d_hidden = lax.dot_general(routed, down_weight, (((1,), (1,)), ((), ())), preferred_element_type=jnp.float32)
    d_upper = (d_hidden * active).astype(jnp.bfloat16)
    d_gate = (d_hidden * upper * sigmoid_gate * (1.0 + gate * (1.0 - sigmoid_gate))).astype(jnp.bfloat16)
    grad_down = lax.dot_general(hidden, routed, (((0,), (0,)), ((), ())), preferred_element_type=jnp.float32).astype(jnp.bfloat16)
    grad_gate = lax.dot_general(inputs, d_gate, (((0,), (0,)), ((), ())), preferred_element_type=jnp.float32).astype(jnp.bfloat16)
    grad_up = lax.dot_general(inputs, d_upper, (((0,), (0,)), ((), ())), preferred_element_type=jnp.float32).astype(jnp.bfloat16)
    return (d_gate, d_upper, grad_gate, grad_up, grad_down)

def input_grad(d_gate, d_upper, gate_weight, up_weight):
    first = lax.dot_general(d_gate, gate_weight, (((1,), (1,)), ((), ())), preferred_element_type=jnp.float32)
    second = lax.dot_general(d_upper, up_weight, (((1,), (1,)), ((), ())), preferred_element_type=jnp.float32)
    return first + second

def gated_pieces(queries, keys, values, log_decay, grad_mix, key_dim, span_len):
    value_dim = values.shape[1] * key_dim // queries.shape[1]
    heads = queries.shape[1] // key_dim
    spans = queries.shape[0] // span_len

    def blocks(array, width):
        return array.astype(jnp.float32).reshape(spans, span_len, heads, width)
    query_spans = blocks(queries, key_dim)
    key_spans = blocks(keys, key_dim)
    value_spans = blocks(values, value_dim)
    grad_spans = blocks(grad_mix, value_dim)
    cumulative = jnp.cumsum(blocks(log_decay, key_dim), axis=1)
    last = cumulative[:, -1]
    scale = key_dim ** (-0.5)
    query_decayed = query_spans * jnp.exp(cumulative)
    key_grown = key_spans * jnp.exp(-cumulative)
    key_to_end = key_spans * jnp.exp(last[:, None] - cumulative)
    g_local = scale * jnp.einsum('nthk,nthv->nhkv', query_decayed, grad_spans, precision=HIGH)
    return (query_spans, key_spans, value_spans, grad_spans, cumulative, last, query_decayed, key_grown, key_to_end, g_local)

def backward_step(carry, inputs):
    local, decay = inputs
    return (local + jnp.exp(decay)[..., None] * carry, carry)

def gated_finish(pieces, span_state, g_end, key_dim):
    query_spans, key_spans, value_spans, grad_spans, cumulative, last, query_decayed, key_grown, key_to_end, g_local = pieces
    spans, span_len, heads, value_dim = value_spans.shape
    scale = key_dim ** (-0.5)
    token_locations = jnp.arange(span_len, dtype=jnp.int32)
    causal = (token_locations[:, None] >= token_locations[None, :]).astype(jnp.float32)
    scores = jnp.einsum('nthk,nshk->nhts', query_decayed, key_grown, precision=HIGH) * causal
    grad_dot = jnp.einsum('nthv,nshv->nhts', grad_spans, value_spans, precision=HIGH) * causal
    state = span_state.astype(jnp.float32).reshape(spans, heads, key_dim, value_dim)
    d_query = scale * jnp.exp(cumulative) * (jnp.einsum('nhts,nshk->nthk', grad_dot, key_grown, precision=HIGH) + jnp.einsum('nthv,nhkv->nthk', grad_spans, state, precision=HIGH))
    d_key = scale * jnp.exp(-cumulative) * jnp.einsum('nhts,nthk->nshk', grad_dot, query_decayed, precision=HIGH) + jnp.exp(last[:, None] - cumulative) * jnp.einsum('nshv,nhkv->nshk', value_spans, g_end, precision=HIGH)
    d_value = scale * jnp.einsum('nhts,nthv->nshv', scores, grad_spans, precision=HIGH) + jnp.einsum('nshk,nhkv->nshv', key_to_end, g_end, precision=HIGH)
    state_end = jnp.exp(last)[..., None] * state + jnp.einsum('nshk,nshv->nhkv', key_to_end, value_spans, precision=HIGH)
    tail = lax.optimization_barrier(jnp.sum(state_end * g_end, axis=-1))
    d_cumulative = query_spans * d_query - key_spans * d_key
    d_log = jnp.cumsum(d_cumulative[:, ::-1], axis=1)[:, ::-1] + tail[:, None]
    rows = spans * span_len
    return (d_query.reshape(rows, heads * key_dim).astype(jnp.bfloat16), d_key.reshape(rows, heads * key_dim).astype(jnp.bfloat16), d_value.reshape(rows, heads * value_dim).astype(jnp.bfloat16), d_log.reshape(rows, heads * key_dim))

def place_block(block):
    return slot_places(block, EXPERTS)

def per_expert(items):
    rows_in, rows_cot, gate_weight, up_weight, down_weight = items
    d_gate, d_upper, grad_gate, grad_up, grad_down = expert_grads(rows_in, rows_cot, gate_weight, up_weight, down_weight)
    return (input_grad(d_gate, d_upper, gate_weight, up_weight), grad_gate, grad_up, grad_down)

def reference(moe_input, cotangent, route_expert, route_weight, w_gate, w_up, w_down, out_proj, saved_out, queries, keys, values, log_decay, span_state):
    blocks = route_expert.reshape(N_SP, TOK_DEV, 2)
    target_locations = jax.vmap(place_block)(blocks)
    source = jnp.arange(N_SP, dtype=jnp.int32)[:, None, None]
    slot_index = (blocks * (N_SP * CAP) + source * CAP + target_locations).reshape(-1).astype(jnp.int32)
    owner = jnp.full((EXPERTS * N_SP * CAP,), 2 * TOKENS, jnp.int32).at[slot_index].set(jnp.arange(2 * TOKENS, dtype=jnp.int32))
    weighted = (route_weight[:, :, None] * cotangent[:, None, :].astype(jnp.float32)).astype(jnp.bfloat16)
    weighted = weighted.reshape(2 * TOKENS, D)
    blank = jnp.zeros((1, D), jnp.bfloat16)
    slot_cot = jnp.concatenate([weighted, blank], axis=0)[owner].reshape(EXPERTS, N_SP * CAP, D)
    slot_in = jnp.concatenate([moe_input, blank], axis=0)[owner // 2].reshape(EXPERTS, N_SP * CAP, D)
    slot_grad, grad_w_gate, grad_w_up, grad_w_down = lax.map(per_expert, (slot_in, slot_cot, w_gate, w_up, w_down))
    routed = slot_grad.reshape(-1, D)[slot_index].reshape(TOKENS, 2, D)
    grad_in = (cotangent.astype(jnp.float32) + routed[:, 0] + routed[:, 1]).astype(jnp.bfloat16)
    grad_mix = lax.dot_general(grad_in, out_proj, (((1,), (1,)), ((), ())), preferred_element_type=jnp.float32)
    grad_proj = lax.dot_general(grad_in, saved_out, (((0,), (0,)), ((), ())), preferred_element_type=jnp.float32)
    pieces = gated_pieces(queries, keys, values, log_decay, grad_mix, DK, SPAN)
    g_local = pieces[9]
    last = pieces[5]
    begin = jnp.zeros((HEADS, DK, DV), jnp.float32)
    ignored, g_end = lax.scan(backward_step, begin, (g_local, last), reverse=True)
    grad_queries, grad_keys, grad_values, grad_decay = gated_finish(pieces, span_state, g_end, DK)
    return (grad_w_gate, grad_w_up, grad_w_down, grad_proj, grad_queries, grad_keys, grad_values, grad_decay)
```

```python
import functools
import math

import jax
import jax.numpy as jnp
from jax import lax
from jax.experimental import pallas as pl
from jax.experimental.pallas import tpu as pltpu
from jax.sharding import PartitionSpec as P

DK = 64
SPAN = 64

HIGH = lax.Precision.HIGHEST
F32 = jnp.float32
BF16 = jnp.bfloat16


def dot(a, b, dims, precision=HIGH):
    return lax.dot_general(
        a, b, ((dims[0], dims[1]), ((), ())), precision=precision, preferred_element_type=F32
    )


NN = ((1,), (0,))
NT = ((1,), (1,))
TN = ((0,), (0,))


def triangle(size, upper):
    row = lax.broadcasted_iota(jnp.int32, (size, size), 0)
    col = lax.broadcasted_iota(jnp.int32, (size, size), 1)
    return ((row <= col) if upper else (row >= col)).astype(F32)


def there(sp=None, tp=None):
    where = {}
    if sp is not None:
        where["sp"] = sp
    if tp is not None:
        where["tp"] = tp
    return where


def greet(partners):
    barrier = pltpu.get_barrier_semaphore()
    for partner in partners:
        pl.semaphore_signal(
            barrier, inc=1, device_id=partner, device_id_type=pl.DeviceIdType.MESH
        )
    pl.semaphore_wait(barrier, len(partners))


def send(src, dst, sems, slot, partner):
    copy = pltpu.make_async_remote_copy(
        src_ref=src,
        dst_ref=dst,
        send_sem=sems[0].at[slot],
        recv_sem=sems[1].at[slot],
        device_id=partner,
        device_id_type=pl.DeviceIdType.MESH,
    )
    copy.start()
    return copy


def expert_kernel(
    n, depth, moe, cot, saved, experts, shares, decay, gate_h, up_h, down_h,
    grad_in, all_s, packet, gate_o, up_o, down_o,
    all_a, all_b, routed, hidden, d_gate, d_upper, gate_w, up_w, down_w,
    slots, got_t, got_p, sum_z, got_z, local, *sems,
):
    me, lane = lax.axis_index("sp"), lax.axis_index("tp")
    core, z = lax.rem(lane, 2), lax.div(lane, 2)
    side = math.isqrt(n)
    y, x = lax.div(me, side), lax.rem(me, side)
    rows, width = moe.shape
    units = hidden.shape[1]
    channels = decay.shape[1]
    split = rows // 2
    wide = width // 2
    part = wide // 2
    piece = rows // depth
    far, near, small, twin_s, plane_s, z_s, back_s, twin_b = (
        sems[2 * i : 2 * i + 2] for i in range(8)
    )

    def ds(start, size):
        return pl.ds(pl.multiple_of(start, size), size)

    def place(dy, dx):
        return lax.rem(y + dy + side, side) * side + lax.rem(x + dx + side, side)

    def half(block):
        return ds(block * rows + core * split, split)

    def whole(block):
        return ds(block * rows, rows)

    started = []

    def go(*args):
        copy = send(*args)
        started.append(copy)
        return copy

    twin = there(tp=lane + 1 - 2 * core)
    peers = [there(sp=lax.rem(me + d, n)) for d in range(1, n)]
    along = [lax.rem(z + d, depth) for d in range(1, depth)]
    lanes = [there(tp=2 * far_z + core) for far_z in along]
    loads = [
        pltpu.make_async_copy(src, dst, local.at[i])
        for i, (src, dst) in enumerate([
            (moe, all_a.at[whole(me)]),
            (cot, all_b.at[whole(me)]),
            (gate_h.at[0], gate_w),
            (up_h.at[0], up_w),
            (down_h.at[0], down_w),
            (saved, all_s.at[whole(me)]),
        ])
    ]
    for load in loads:
        load.start()
    index = lax.broadcasted_iota(jnp.int32, (n, rows), 0)
    packet[me, 0:n, :] = jnp.where(index == experts[0:1, :], shares[0:1, :], 0.0) + jnp.where(
        index == experts[1:2, :], shares[1:2, :], 0.0
    )
    packet[me, n : n + 1, 0:channels] = jnp.sum(decay[...], axis=0, keepdims=True)
    greet(peers + lanes + [twin])
    notes = [
        go(packet.at[me], packet.at[me], small, d, peer) for d, peer in enumerate(peers)
    ]
    loads[0].wait()
    loads[1].wait()
    offsets = range(1, side)
    reach = side - 1
    first = {}
    for turn, (on_x, on_y) in enumerate([(all_b, all_a), (all_a, all_b)]):
        for d in offsets:
            base, at = 2 * turn * reach + d - 1, half(me)
            first["x", turn, d] = go(
                on_x.at[at], on_x.at[at], far, base, there(sp=place(0, d))
            )
            first["y", turn, d] = go(
                on_y.at[at], on_y.at[at], far, base + reach, there(sp=place(d, 0))
            )
    eye = lax.broadcasted_iota(jnp.int32, (rows, rows), 0) == lax.broadcasted_iota(
        jnp.int32, (rows, rows), 1
    )
    tile = 256 if units % 256 == 0 else 128
    own, other = ds(core * wide, wide), ds((1 - core) * wide, wide)

    def relay(copy, full, block, slot):
        copy.wait_recv()
        at = half(block)
        return go(full.at[at], full.at[at], near, slot, twin)

    def expert(block):
        at = whole(block)
        line = packet[block, pl.ds(me, 1), :]
        scale = jnp.sum(jnp.where(eye, line, 0.0), axis=1, keepdims=True)
        routed[at, :] = (all_b[at, :].astype(F32) * scale).astype(BF16)
        for start in range(0, units, tile):
            j = slice(start, start + tile)
            gate = dot(all_a[at, :], gate_w[:, j], NN, None)
            upper = dot(all_a[at, :], up_w[:, j], NN, None)
            d_hidden = dot(routed[at, :], down_w[j, :], NT, None)
            sigmoid_gate = jax.nn.sigmoid(gate)
            active = gate * sigmoid_gate
            hidden[at, j] = (active * upper).astype(BF16)
            d_upper[at, j] = (d_hidden * active).astype(BF16)
            d_gate[at, j] = (
                d_hidden * upper * sigmoid_gate * (1.0 + gate * (1.0 - sigmoid_gate))
            ).astype(BF16)

    def back(block, which):
        at = whole(block)
        for j in range(0, wide, 256):
            to = ds(which * wide + j, 256)
            slots[at, to] = (
                dot(d_gate[at, :], gate_w[to, :], NT, None)
                + dot(d_upper[at, :], up_w[to, :], NT, None)
            ).astype(BF16)

    crossing = {}

    def emit(dy, dx):
        block = place(dy, dx)
        slot = (dy % side) * side + dx % side
        expert(block)
        back(block, 1 - core)
        copy = go(slots.at[whole(block), other], got_t.at[slot], twin_s, slot, twin)
        back(block, core)
        copy.wait_recv()
        got_t[slot] = (
            slots[whole(block), own].astype(F32) + got_t[slot].astype(F32)
        ).astype(BF16)
        if slot:
            for h in range(2):
                cut = slice(h * part, (h + 1) * part)
                crossing[slot, h] = go(
                    got_t.at[slot, :, cut], got_p.at[slot - 1, :, cut], plane_s,
                    2 * (slot - 1) + h, there(sp=block),
                )

    for load in loads[2:5]:
        load.wait()
    emit(0, 0)
    second, passed = {}, {}
    flat = 4 * reach
    square = reach * reach
    for d in offsets:
        passed["y", 0, d] = relay(first["y", 0, d], all_a, place(-d, 0), reach + d - 1)
        at = half(place(-d, 0))
        for e in offsets:
            second[0, d, e] = go(
                all_a.at[at], all_a.at[at], far, flat + (d - 1) * reach + e - 1,
                there(sp=place(0, e)),
            )
        passed["x", 0, d] = relay(first["x", 0, d], all_b, place(0, -d), d - 1)
        at = half(place(0, -d))
        for e in offsets:
            second[1, e, d] = go(
                all_b.at[at], all_b.at[at], far, flat + square + (e - 1) * reach + d - 1,
                there(sp=place(e, 0)),
            )
    loads[5].wait()
    at = whole(me)
    shared = [
        go(all_s.at[at], all_s.at[at], small, n - 1 + d, peer)
        for d, peer in enumerate(peers)
    ]
    for d in offsets:
        passed["x", 1, d] = relay(first["x", 1, d], all_a, place(0, -d), 2 * reach + d - 1)
        passed["y", 1, d] = relay(first["y", 1, d], all_b, place(-d, 0), 3 * reach + d - 1)
    for note in notes:
        note.wait_recv()
    for d in offsets:
        for turn in range(2):
            passed["x", turn, d].wait_recv()
        emit(0, -d)
        for turn in range(2):
            passed["y", turn, d].wait_recv()
        emit(-d, 0)
    for d in offsets:
        for e in offsets:
            base = flat + (d - 1) * reach + e - 1
            pair = [
                relay(second[0, d, e], all_a, place(-d, -e), base),
                relay(second[1, d, e], all_b, place(-d, -e), base + square),
            ]
            for copy in pair:
                copy.wait_recv()
            emit(-d, -e)

    def gate_up(i, carry):
        at = ds(i * 256, 256)
        gate_o[0, at, :] = dot(all_a[:, at], d_gate[...], TN, None).astype(BF16)
        up_o[0, at, :] = dot(all_a[:, at], d_upper[...], TN, None).astype(BF16)
        return carry

    def down(i, carry):
        at = ds(i * 256, 256)
        down_o[0, :, at] = dot(hidden[...], routed[:, at], TN, None).astype(BF16)
        return carry

    steps = width // 256
    lax.fori_loop(0, steps // 2, gate_up, 0)
    third, fourth, fifth = {}, {}, []
    for h in range(2):
        cut = slice(h * part, (h + 1) * part)
        total = got_t[0, :, cut].astype(F32)
        for slot in range(1, n):
            crossing[slot, h].wait_recv()
            total = total + got_p[slot - 1, :, cut].astype(F32)
        sum_z[:, cut] = total.astype(BF16)
        for d in range(depth - 1):
            third[h, d] = go(
                sum_z.at[ds(along[d] * piece, piece), cut], got_z.at[d, :, cut], z_s,
                h * (depth - 1) + d, lanes[d],
            )
    lax.fori_loop(steps // 2, steps, gate_up, 0)
    kept = ds(z * piece, piece)
    for h in range(2):
        cut = slice(h * part, (h + 1) * part)
        to = ds(core * wide + h * part, part)
        total = all_b[ds(me * rows + z * piece, piece), to].astype(F32)
        total = total + sum_z[kept, cut].astype(F32)
        for d in range(depth - 1):
            third[h, d].wait_recv()
            total = total + got_z[d, :, cut].astype(F32)
        grad_in[kept, to] = total.astype(BF16)
        for d in range(depth - 1):
            fourth[h, d] = go(
                grad_in.at[kept, to], grad_in.at[kept, to], back_s,
                h * (depth - 1) + d, lanes[d],
            )
        fifth.append(
            go(grad_in.at[kept, to], grad_in.at[kept, to], twin_b, h * depth, twin)
        )
    lax.fori_loop(0, steps, down, 0)
    for h in range(2):
        to = ds(core * wide + h * part, part)
        for d in range(depth - 1):
            fourth[h, d].wait_recv()
            at = ds(lax.rem(z + depth - 1 - d, depth) * piece, piece)
            fifth.append(
                go(grad_in.at[at, to], grad_in.at[at, to], twin_b, h * depth + d + 1, twin)
            )
    for copy in shared + fifth:
        copy.wait_recv()
    for copy in started:
        copy.wait_send()


def mix_kernel(
    n, grad_in, out_proj, queries, log_decay, packet, mix_out, after, proj_in, starts, *sems
):
    me, lane = lax.axis_index("sp"), lax.axis_index("tp")
    core = lax.rem(lane, 2)
    twin = there(tp=lane + 1 - 2 * core)
    peers = [there(sp=lax.rem(me + d, n)) for d in range(1, n)]
    rows, width = grad_in.shape
    part = width // n
    split = rows // 2
    far, near, begin = (sems[2 * i : 2 * i + 2] for i in range(3))

    def ds(start, size):
        return pl.ds(pl.multiple_of(start, size), size)

    greet(peers + [twin])
    ours = []
    for d, peer in enumerate(peers):
        to = lax.rem(me + d + 1, n)
        ours.append(send(
            grad_in.at[ds(core * split, split), ds(to * part, part)],
            proj_in.at[ds(me * rows + core * split, split)], far, d, peer,
        ))
    proj_in[ds(me * rows, rows), :] = grad_in[:, ds(me * part, part)]
    mix = dot(grad_in[...], out_proj[...], NT, None)
    mix_out[...] = mix
    channels = queries.shape[1]
    heads = channels // DK
    wide = mix.shape[1] // heads
    lower = triangle(SPAN, False)
    ones = jnp.ones((SPAN, wide), F32)
    for h in range(heads):
        keyed = slice(h * DK, (h + 1) * DK)
        carry = None
        for n_ in reversed(range(rows // SPAN)):
            at = slice(n_ * SPAN, (n_ + 1) * SPAN)
            decay = log_decay[at, keyed]
            qd = queries[at, keyed].astype(F32) * jnp.exp(dot(lower, decay, NN))
            local = DK**-0.5 * dot(qd, mix[at, h * wide : (h + 1) * wide], TN)
            if carry is not None:
                local = local + jnp.exp(dot(decay, ones, TN)) * carry
            carry = local
        starts[me, keyed, :] = carry
    copies = [send(starts.at[me], starts.at[me], begin, d, peers[d]) for d in range(n - 1)]
    relayed = []
    for d in range(n - 1):
        ours[d].wait_recv()
        source = lax.rem(me + n - 1 - d, n)
        at = ds(source * rows + core * split, split)
        relayed.append(send(proj_in.at[at], proj_in.at[at], near, d, twin))
    index = lax.broadcasted_iota(jnp.int32, (n, channels), 0)
    decays = jnp.concatenate([packet[q, n : n + 1, 0:channels] for q in range(n)], axis=0)
    lanes = jnp.ones((n, wide), F32)
    total = jnp.zeros((channels, wide), F32)
    for d in range(n - 1):
        copies[d].wait_recv()
        source = lax.rem(me + n - 1 - d, n)
        passed = jnp.where((index > me) & (index < source), decays, 0.0)
        factor = jnp.exp(dot(passed, lanes, TN))
        total = total + jnp.where(source > me, factor, 0.0) * starts[source]
    after[...] = total
    for copy in relayed:
        copy.wait_recv()
    for copy in ours + copies + relayed:
        copy.wait_send()


def finish_kernel(queries, keys, values, log_decay, mix, state, after, dq_o, dk_o, dv_o, dl_o):
    rows, channels = queries.shape
    heads = channels // DK
    wide = values.shape[1] // heads
    lower = triangle(SPAN, False)
    upper = triangle(SPAN, True)
    ones = jnp.ones((SPAN, wide), F32)
    scale = DK**-0.5
    for h in range(heads):
        keyed = slice(h * DK, (h + 1) * DK)
        valued = slice(h * wide, (h + 1) * wide)
        g_end = after[keyed, :]
        for n in reversed(range(rows // SPAN)):
            at = slice(n * SPAN, (n + 1) * SPAN)
            q = queries[at, keyed].astype(F32)
            k = keys[at, keyed].astype(F32)
            v = values[at, valued].astype(F32)
            g = mix[at, valued]
            s0 = state[n, keyed, :]
            decay = log_decay[at, keyed]
            c = dot(lower, decay, NN)
            last = c[SPAN - 1 : SPAN, :]
            grow, shrink, to_end = jnp.exp(c), jnp.exp(-c), jnp.exp(last - c)
            qd, kd, ke = q * grow, k * shrink, k * to_end
            scores = dot(qd, kd, NT) * lower
            gv = dot(g, v, NT) * lower
            dq = scale * grow * (dot(gv, kd, NN) + dot(g, s0, NT))
            dk = scale * shrink * dot(gv, qd, TN) + to_end * dot(v, g_end, NT)
            dv = scale * dot(scores, g, TN) + dot(ke, g_end, NN)
            e_last = jnp.exp(dot(decay, ones, TN))
            s1 = e_last * s0 + dot(ke, v, TN)
            dq_o[at, keyed] = dq.astype(BF16)
            dk_o[at, keyed] = dk.astype(BF16)
            dv_o[at, valued] = dv.astype(BF16)
            dl_o[at, keyed] = dot(upper, q * dq - k * dk, NN) + dot(ones, s1 * g_end, NT)
            if n:
                g_end = DK**-0.5 * dot(qd, g, TN) + e_last * g_end


def last_kernel(
    gate, up, down, proj_in, all_s, queries, keys, values, log_decay, mix, state, after,
    gate_o, up_o, down_o, proj_o, dq_o, dk_o, dv_o, dl_o, sems,
):
    stores = [
        pltpu.make_async_copy(src, dst, sems.at[i])
        for i, (src, dst) in enumerate([(gate, gate_o), (up, up_o), (down, down_o)])
    ]
    for store in stores:
        store.start()
    proj_o[...] = dot(proj_in[...], all_s[...], TN, None)
    finish_kernel(
        queries, keys, values, log_decay, mix, state, after, dq_o, dk_o, dv_o, dl_o
    )
    for store in stores:
        store.wait()


def size_of(scratch):
    return sum(math.prod(s) * jnp.dtype(d).itemsize for s, d in scratch)


def call(kernel, outs, ins, args, scratch=(), sems=(), ident=None, flops=2 * 10**8):
    semaphores = [pltpu.SemaphoreType.DMA((count,)) for count in sems]
    limit = size_of(scratch) + (8 << 20)
    return pl.pallas_call(
        kernel,
        out_shape=[
            jax.ShapeDtypeStruct(s, d) if m == pl.ANY else m(s, d) for m, s, d in outs
        ],
        in_specs=[pl.BlockSpec(memory_space=m) for m in ins],
        out_specs=[pl.BlockSpec(memory_space=m) for m, s, d in outs],
        scratch_shapes=[pltpu.VMEM(s, d) for s, d in scratch] + semaphores,
        cost_estimate=pl.CostEstimate(flops=flops, bytes_accessed=10**6, transcendentals=0),
        compiler_params=pltpu.CompilerParams(
            collective_id=ident, has_side_effects=ident is not None, vmem_limit_bytes=limit
        ),
    )(*args)


def on_device(
    moe_input,
    cotangent,
    route_expert,
    route_weight,
    w_gate,
    w_up,
    w_down,
    out_proj,
    saved_out,
    queries,
    keys,
    values,
    log_decay,
    span_state,
):
    rows, width = moe_input.shape
    groups = lax.axis_size("sp")
    depth = lax.axis_size("tp") // 2
    units = w_gate.shape[2]
    tokens = groups * rows
    channels, wide = queries.shape[1], span_state.shape[2]
    lanes = values.shape[1]
    fast, slow = pltpu.VMEM, pl.ANY
    packet_rows = -(-(groups + 1) // 8) * 8
    reach = math.isqrt(groups) - 1
    links = 4 * reach + 2 * reach * reach

    def both(*counts):
        return [count for count in counts for _ in range(2)]

    grad_in, all_s, packet, gate_v, up_v, down_v = call(
        functools.partial(expert_kernel, groups, depth),
        [
            (fast, (rows, width), BF16),
            (fast, (tokens, lanes), BF16),
            (fast, (groups, packet_rows, rows), F32),
            (fast, w_gate.shape, BF16),
            (fast, w_up.shape, BF16),
            (fast, w_down.shape, BF16),
        ],
        [slow, slow, slow, fast, fast, fast, slow, slow, slow],
        (
            moe_input, cotangent, saved_out, route_expert.T, route_weight.T, log_decay,
            w_gate, w_up, w_down,
        ),
        scratch=[
            ((tokens, width), BF16),
            ((tokens, width), BF16),
            ((tokens, width), BF16),
            ((tokens, units), BF16),
            ((tokens, units), BF16),
            ((tokens, units), BF16),
            ((width, units), BF16),
            ((width, units), BF16),
            ((units, width), BF16),
            ((tokens, width), BF16),
            ((groups, rows, width // 2), BF16),
            ((groups - 1, rows, width // 2), BF16),
            ((rows, width // 2), BF16),
            ((depth - 1, rows // depth, width // 2), BF16),
        ],
        sems=[6] + both(
            links, links, 2 * (groups - 1), groups, 2 * (groups - 1), 2 * (depth - 1),
            2 * (depth - 1), 2 * depth,
        ),
        ident=1,
        flops=10**10,
    )
    mix, after, proj_in = call(
        functools.partial(mix_kernel, groups),
        [
            (fast, (rows, lanes), F32),
            (fast, (channels, wide), F32),
            (fast, (tokens, width // groups), BF16),
        ],
        [fast] * 5,
        (grad_in, out_proj, queries, log_decay, packet),
        scratch=[((groups, channels, wide), F32)],
        sems=both(groups - 1, groups - 1, groups - 1),
        ident=2,
    )
    return call(
        last_kernel,
        [
            (slow, w_gate.shape, BF16),
            (slow, w_up.shape, BF16),
            (slow, w_down.shape, BF16),
            (fast, (width // groups, lanes), F32),
            (fast, queries.shape, BF16),
            (fast, keys.shape, BF16),
            (fast, values.shape, BF16),
            (fast, log_decay.shape, F32),
        ],
        [fast] * 12,
        (
            gate_v, up_v, down_v, proj_in, all_s, queries, keys, values, log_decay, mix,
            span_state, after,
        ),
        sems=[3],
    )


def solution(mesh):
    placed = (
        P("sp", None),
        P("sp", None),
        P("sp", None),
        P("sp", None),
        P("sp", None, "tp"),
        P("sp", None, "tp"),
        P("sp", "tp", None),
        P("tp", None),
        P("sp", "tp"),
        P("sp", "tp"),
        P("sp", "tp"),
        P("sp", "tp"),
        P("sp", "tp"),
        P("sp", "tp", None),
    )
    return jax.shard_map(
        on_device,
        mesh=mesh,
        in_specs=placed,
        out_specs=(
            P("sp", None, "tp"),
            P("sp", None, "tp"),
            P("sp", "tp", None),
            P("sp", "tp"),
            P("sp", "tp"),
            P("sp", "tp"),
            P("sp", "tp"),
            P("sp", "tp"),
        ),
        check_vma=False,
    )
```

```python
import functools
import math

import jax
import jax.numpy as jnp
from jax import lax
from jax.experimental import pallas as pl
from jax.experimental.pallas import tpu as pltpu
from jax.sharding import PartitionSpec as P

DK = 64
SPAN = 64
CUTS = 2

HIGH = lax.Precision.HIGHEST
F32 = jnp.float32
BF16 = jnp.bfloat16


def dot(a, b, dims, precision=HIGH):
    return lax.dot_general(
        a, b, ((dims[0], dims[1]), ((), ())), precision=precision, preferred_element_type=F32
    )


NN = ((1,), (0,))
NT = ((1,), (1,))
TN = ((0,), (0,))


def triangle(size, upper):
    row = lax.broadcasted_iota(jnp.int32, (size, size), 0)
    col = lax.broadcasted_iota(jnp.int32, (size, size), 1)
    return ((row <= col) if upper else (row >= col)).astype(F32)


def there(sp=None, tp=None):
    where = {}
    if sp is not None:
        where["sp"] = sp
    if tp is not None:
        where["tp"] = tp
    return where


def greet(partners):
    barrier = pltpu.get_barrier_semaphore()
    for partner in partners:
        pl.semaphore_signal(
            barrier, inc=1, device_id=partner, device_id_type=pl.DeviceIdType.MESH
        )
    pl.semaphore_wait(barrier, len(partners))


def send(src, dst, sems, slot, partner):
    copy = pltpu.make_async_remote_copy(
        src_ref=src,
        dst_ref=dst,
        send_sem=sems[0].at[slot],
        recv_sem=sems[1].at[slot],
        device_id=partner,
        device_id_type=pl.DeviceIdType.MESH,
    )
    copy.start()
    return copy


def expert_kernel(
    n, depth, moe, cot, saved, experts_h, shares_h, decay_h, gate_h, up_h, down_h,
    out_h, query_h, key_h, value_h, state_h,
    gate_o, up_o, down_o, all_s, proj_in, after, mid, fall, ends, to_end, ke, dq_o, dk_o, dv_o,
    grad_in, packet, out_proj, queries, keys, values, state, starts, factors,
    grow, shrink, qd, kd, scores,
    all_a, all_b, routed, hidden, d_gate, d_upper, gate_w, up_w,
    gate_t, up_t, down_t,
    slots, mine, got_t, got_p, sum_z, got_z, experts, shares, decay, local, *sems,
):
    me, lane = lax.axis_index("sp"), lax.axis_index("tp")
    core, z = lax.rem(lane, 2), lax.div(lane, 2)
    side = math.isqrt(n)
    y, x = lax.div(me, side), lax.rem(me, side)
    rows, width = moe.shape
    units = hidden.shape[1]
    channels = decay.shape[1]
    split = rows // 2
    wide = width // 2
    cuts = CUTS
    part = wide // cuts
    piece = rows // depth
    far, near, small, twin_s, plane_s, z_s, back_s, twin_b, slice_s, slice_t, begin = (
        sems[2 * i : 2 * i + 2] for i in range(11)
    )

    def ds(start, size):
        return pl.ds(pl.multiple_of(start, size), size)

    def place(dy, dx):
        return lax.rem(y + dy + side, side) * side + lax.rem(x + dx + side, side)

    def half(block):
        return ds(block * rows + core * split, split)

    def whole(block):
        return ds(block * rows, rows)

    started = []

    def go(*args):
        copy = send(*args)
        started.append(copy)
        return copy

    twin = there(tp=lane + 1 - 2 * core)
    peers = [there(sp=lax.rem(me + d, n)) for d in range(1, n)]
    along = [lax.rem(z + d, depth) for d in range(1, depth)]
    lanes = [there(tp=2 * far_z + core) for far_z in along]
    loads = [
        pltpu.make_async_copy(src, dst, local.at[i])
        for i, (src, dst) in enumerate([
            (moe, all_a.at[whole(me)]),
            (cot, all_b.at[whole(me)]),
            (gate_h.at[0], gate_w),
            (up_h.at[0], up_w),
            (down_h.at[0], down_o.at[0]),
            (saved, all_s.at[whole(me)]),
            (experts_h, experts),
            (shares_h, shares),
            (decay_h, decay),
            (query_h, queries),
            (key_h, keys),
            (value_h, values),
            (state_h, state),
            (out_h, out_proj),
        ])
    ]
    for load in loads[6:9] + loads[:6] + loads[9:]:
        load.start()
    for load in loads[6:9]:
        load.wait()
    index = lax.broadcasted_iota(jnp.int32, (n, rows), 0)
    packet[me, 0:n, :] = jnp.where(index == experts[0:1, :], shares[0:1, :], 0.0) + jnp.where(
        index == experts[1:2, :], shares[1:2, :], 0.0
    )
    packet[me, n : n + 1, 0:channels] = jnp.sum(decay[...], axis=0, keepdims=True)
    greet(peers + lanes + [twin])
    notes = [
        go(packet.at[me], packet.at[me], small, d, peer) for d, peer in enumerate(peers)
    ]
    loads[0].wait()
    loads[1].wait()
    offsets = range(1, side)
    reach = side - 1
    first = {}
    for turn, (on_x, on_y) in enumerate([(all_b, all_a), (all_a, all_b)]):
        for d in offsets:
            base, at = 2 * turn * reach + d - 1, half(me)
            first["x", turn, d] = go(
                on_x.at[at], on_x.at[at], far, base, there(sp=place(0, d))
            )
            first["y", turn, d] = go(
                on_y.at[at], on_y.at[at], far, base + reach, there(sp=place(d, 0))
            )
    eye = lax.broadcasted_iota(jnp.int32, (rows, rows), 0) == lax.broadcasted_iota(
        jnp.int32, (rows, rows), 1
    )
    tile = 256 if units % 256 == 0 else 128

    def relay(copy, full, block, slot):
        copy.wait_recv()
        at = half(block)
        return go(full.at[at], full.at[at], near, slot, twin)

    def turn_over(src, dst):
        columns = src.shape[1]
        strip = 256 if columns % 256 == 0 else 128

        def step(i, carry):
            at = ds(i * 256, 256)
            for j in range(0, columns, strip):
                dst[j : j + strip, at] = src[at, j : j + strip].T
            return carry

        lax.fori_loop(0, src.shape[0] // 256, step, 0)

    def rows_of(ref, blocks):
        parts = [ref[whole(block), :] for block in blocks]
        return parts[0] if len(parts) == 1 else jnp.concatenate(parts, axis=0)

    def expert(blocks):
        for block in blocks:
            at = whole(block)
            line = packet[block, pl.ds(me, 1), :]
            scale = jnp.sum(jnp.where(eye, line, 0.0), axis=1, keepdims=True)
            routed[at, :] = (all_b[at, :].astype(F32) * scale).astype(BF16)
        for start in range(0, units, tile):
            j = slice(start, start + tile)
            gate = dot(rows_of(all_a, blocks), gate_w[:, j], NN, None)
            upper = dot(rows_of(all_a, blocks), up_w[:, j], NN, None)
            d_hidden = dot(rows_of(routed, blocks), down_t[:, j], NN, None)
            sigmoid_gate = jax.nn.sigmoid(gate)
            active = gate * sigmoid_gate
            made = [
                (hidden, active * upper),
                (d_upper, d_hidden * active),
                (
                    d_gate,
                    d_hidden * upper * sigmoid_gate * (1.0 + gate * (1.0 - sigmoid_gate)),
                ),
            ]
            for ref, value in made:
                for i, block in enumerate(blocks):
                    ref[whole(block), j] = value[i * rows : (i + 1) * rows].astype(BF16)

    def back(blocks, which):
        for j in range(0, wide, 256):
            to = ds(which * wide + j, 256)
            value = dot(rows_of(d_gate, blocks), gate_t[:, to], NN, None) + dot(
                rows_of(d_upper, blocks), up_t[:, to], NN, None
            )
            yield slice(j, j + 256), value

    wide_v = values.shape[1]
    heads = channels // DK
    value_dim = wide_v // heads
    spans = rows // SPAN
    row = lax.broadcasted_iota(jnp.int32, (rows, rows), 0)
    col = lax.broadcasted_iota(jnp.int32, (rows, rows), 1)
    causal = (row >= col) & (lax.div(row, SPAN) == lax.div(col, SPAN))

    def keyed(h):
        return slice(h * DK, (h + 1) * DK)

    def valued(h):
        return slice(h * value_dim, (h + 1) * value_dim)

    def span(i):
        return slice(i * SPAN, (i + 1) * SPAN)

    def prepare():
        c = dot(causal.astype(F32), decay[...], NN)
        ones = jnp.ones((SPAN, value_dim), F32)
        grow[...] = jnp.exp(c)
        shrink[...] = jnp.exp(-c)
        for i in range(spans):
            at = span(i)
            last = c[(i + 1) * SPAN - 1 : (i + 1) * SPAN, :]
            to_end[at, :] = jnp.exp(last - c[at, :])
            fall[i] = jnp.exp(dot(decay[at, :], ones, TN))
        qd[...] = (queries[...].astype(F32) * grow[...]).astype(BF16)
        kd[...] = (keys[...].astype(F32) * shrink[...]).astype(BF16)
        ke[...] = (keys[...].astype(F32) * to_end[...]).astype(BF16)
        for h in range(heads):
            scores[h] = jnp.where(
                causal, dot(qd[:, keyed(h)], kd[:, keyed(h)], NT, None), 0.0
            ).astype(BF16)
            for i in range(spans):
                ends[i, keyed(h), :] = fall[i, keyed(h), :] * state[i, keyed(h), :] + dot(
                    ke[span(i), keyed(h)], values[span(i), valued(h)], TN, None
                )

    crossing = {}

    def emit(*steps):
        blocks = [place(dy, dx) for dy, dx in steps]
        marks = [(dy % side) * side + dx % side for dy, dx in steps]
        expert(blocks)
        for cut, value in back(blocks, 1 - core):
            for i, block in enumerate(blocks):
                slots[whole(block), cut] = value[i * rows : (i + 1) * rows].astype(BF16)
        swaps = [
            go(slots.at[whole(block)], got_t.at[slot], twin_s, slot, twin)
            for block, slot in zip(blocks, marks)
        ]
        for cut, value in back(blocks, core):
            mine[0 : len(blocks) * rows, cut] = value
        for i, (block, slot, copy) in enumerate(zip(blocks, marks, swaps)):
            copy.wait_recv()
            got_t[slot] = (
                mine[i * rows : (i + 1) * rows, :] + got_t[slot].astype(F32)
            ).astype(BF16)
            for h in range(cuts if slot else 0):
                cut = slice(h * part, (h + 1) * part)
                crossing[slot, h] = go(
                    got_t.at[slot, :, cut], got_p.at[slot - 1, :, cut], plane_s,
                    cuts * (slot - 1) + h, there(sp=block),
                )

    for load in loads[9:]:
        load.wait()
    prepare()
    for load in loads[2:5]:
        load.wait()
    turn_over(down_o.at[0], down_t)
    turn_over(gate_w, gate_t)
    turn_over(up_w, up_t)
    second, passed = {}, {}
    flat = 4 * reach
    square = reach * reach
    for d in offsets:
        passed["y", 0, d] = relay(first["y", 0, d], all_a, place(-d, 0), reach + d - 1)
        at = half(place(-d, 0))
        for e in offsets:
            second[0, d, e] = go(
                all_a.at[at], all_a.at[at], far, flat + (d - 1) * reach + e - 1,
                there(sp=place(0, e)),
            )
        passed["x", 0, d] = relay(first["x", 0, d], all_b, place(0, -d), d - 1)
        at = half(place(0, -d))
        for e in offsets:
            second[1, e, d] = go(
                all_b.at[at], all_b.at[at], far, flat + square + (e - 1) * reach + d - 1,
                there(sp=place(e, 0)),
            )
    emit((0, 0))
    for d in offsets:
        passed["x", 1, d] = relay(first["x", 1, d], all_a, place(0, -d), 2 * reach + d - 1)
        passed["y", 1, d] = relay(first["y", 1, d], all_b, place(-d, 0), 3 * reach + d - 1)
    for note in notes:
        note.wait_recv()
    order = lax.broadcasted_iota(jnp.int32, (n, channels), 0)
    decays = jnp.concatenate([packet[q, n : n + 1, 0:channels] for q in range(n)], axis=0)
    for d in range(n - 1):
        source = lax.rem(me + n - 1 - d, n)
        between = jnp.where((order > me) & (order < source), decays, 0.0)
        factor = jnp.exp(dot(between, jnp.ones((n, value_dim), F32), TN))
        factors[d] = jnp.where(source > me, factor, 0.0)
    for d in offsets:
        for turn in range(2):
            passed["x", turn, d].wait_recv()
            passed["y", turn, d].wait_recv()
        emit((0, -d), (-d, 0))
    for d in offsets:
        for e in offsets:
            base = flat + (d - 1) * reach + e - 1
            pair = [
                relay(second[0, d, e], all_a, place(-d, -e), base),
                relay(second[1, d, e], all_b, place(-d, -e), base + square),
            ]
            for copy in pair:
                copy.wait_recv()
            emit((-d, -e))

    def gate_up(i, carry):
        at = ds(i * 256, 256)
        gate_o[0, at, :] = dot(all_a[:, at], d_gate[...], TN, None).astype(BF16)
        up_o[0, at, :] = dot(all_a[:, at], d_upper[...], TN, None).astype(BF16)
        return carry

    def down(i, carry):
        at = ds(i * tile, tile)
        turned = hidden[:, at].T
        for j in range(0, width, 512):
            to = slice(j, j + 512)
            down_o[0, at, to] = dot(turned, routed[:, to], NN, None).astype(BF16)
        return carry

    steps = width // 256
    turns = units // tile
    lax.fori_loop(0, steps, gate_up, 0)
    third, fourth, fifth = {}, {}, []
    for h in range(cuts):
        cut = slice(h * part, (h + 1) * part)
        total = got_t[0, :, cut].astype(F32)
        for slot in range(1, n):
            crossing[slot, h].wait_recv()
            total = total + got_p[slot - 1, :, cut].astype(F32)
        sum_z[:, cut] = total.astype(BF16)
        for d in range(depth - 1):
            third[h, d] = go(
                sum_z.at[ds(along[d] * piece, piece), cut], got_z.at[d, :, cut], z_s,
                h * (depth - 1) + d, lanes[d],
            )
    loads[5].wait()
    at = whole(me)
    shared = [
        go(all_s.at[at], all_s.at[at], small, n - 1 + d, peer)
        for d, peer in enumerate(peers)
    ]
    lax.fori_loop(0, turns // 2, down, 0)
    kept = ds(z * piece, piece)
    for h in range(cuts):
        cut = slice(h * part, (h + 1) * part)
        to = ds(core * wide + h * part, part)
        total = all_b[ds(me * rows + z * piece, piece), to].astype(F32)
        total = total + sum_z[kept, cut].astype(F32)
        for d in range(depth - 1):
            third[h, d].wait_recv()
            total = total + got_z[d, :, cut].astype(F32)
        grad_in[kept, to] = total.astype(BF16)
        for d in range(depth - 1):
            fourth[h, d] = go(
                grad_in.at[kept, to], grad_in.at[kept, to], back_s,
                h * (depth - 1) + d, lanes[d],
            )
        fifth.append(
            go(grad_in.at[kept, to], grad_in.at[kept, to], twin_b, h * depth, twin)
        )
    lax.fori_loop(turns // 2, turns, down, 0)
    for h in range(cuts):
        to = ds(core * wide + h * part, part)
        for d in range(depth - 1):
            fourth[h, d].wait_recv()
            at = ds(lax.rem(z + depth - 1 - d, depth) * piece, piece)
            fifth.append(
                go(grad_in.at[at, to], grad_in.at[at, to], twin_b, h * depth + d + 1, twin)
            )
    for copy in fifth:
        copy.wait_recv()
    slab = width // n
    mix = dot(grad_in[...], out_proj[...], NT, None)
    g = mix.astype(BF16)
    scale = DK**-0.5
    for h in range(heads):
        carry = None
        for i in reversed(range(spans)):
            local_g = scale * dot(qd[span(i), keyed(h)], g[span(i), valued(h)], TN, None)
            mid[i, keyed(h), :] = local_g
            carry = local_g if carry is None else local_g + fall[i, keyed(h), :] * carry
        starts[me, keyed(h), :] = carry.astype(BF16)
    opened = [go(starts.at[me], starts.at[me], begin, d, peers[d]) for d in range(n - 1)]
    sliced = [
        go(
            grad_in.at[ds(core * split, split), ds(lax.rem(me + d + 1, n) * slab, slab)],
            proj_in.at[half(me)], slice_s, d, peer,
        )
        for d, peer in enumerate(peers)
    ]
    proj_in[whole(me), :] = grad_in[:, ds(me * slab, slab)]
    for h in range(heads):
        gh = g[:, valued(h)]
        gv = jnp.where(causal, dot(gh, values[:, valued(h)], NT, None), 0.0).astype(BF16)
        past = jnp.concatenate([
            dot(gh[span(i), :], state[i, keyed(h), :].astype(BF16), NT, None)
            for i in range(spans)
        ], axis=0)
        dq_o[:, keyed(h)] = scale * grow[:, keyed(h)] * (
            dot(gv, kd[:, keyed(h)], NN, None) + past
        )
        dk_o[:, keyed(h)] = scale * shrink[:, keyed(h)] * dot(gv, qd[:, keyed(h)], TN, None)
        dv_o[:, valued(h)] = scale * dot(scores[h], gh, TN, None)
    total = jnp.zeros((channels, value_dim), F32)
    for d in range(n - 1):
        opened[d].wait_recv()
        total = total + factors[d] * starts[lax.rem(me + n - 1 - d, n)].astype(F32)
    after[...] = total
    relayed = []
    for d in range(n - 1):
        sliced[d].wait_recv()
        at = half(lax.rem(me + n - 1 - d, n))
        relayed.append(go(proj_in.at[at], proj_in.at[at], slice_t, d, twin))
    for copy in shared + relayed:
        copy.wait_recv()
    for copy in started:
        copy.wait_send()


def last_kernel(
    gate, up, down, all_s, proj_in, after, mid, fall, ends, to_end, ke, dq, dk_p, dv_p,
    queries, keys, values,
    gate_o, up_o, down_o, proj_o, dq_o, dk_o, dv_o, dl_o,
    proj_v, dq_v, dk_v, dv_v, dl_v, sems,
):
    stores = []

    def store(src, dst):
        copy = pltpu.make_async_copy(src, dst, sems.at[len(stores)])
        copy.start()
        stores.append(copy)

    for src, dst in [(gate, gate_o), (up, up_o), (down, down_o)]:
        store(src, dst)
    dq_v[...] = dq[...].astype(BF16)
    store(dq_v, dq_o)
    rows, channels = queries.shape
    heads = channels // DK
    wide = values.shape[1] // heads
    ones = jnp.ones((SPAN, wide), F32)
    upper = triangle(SPAN, True)
    g_end = after[...]
    for n in reversed(range(rows // SPAN)):
        at = slice(n * SPAN, (n + 1) * SPAN)
        narrow = g_end.astype(BF16)
        grown = ends[n] * g_end
        for h in range(heads):
            keyed = slice(h * DK, (h + 1) * DK)
            valued = slice(h * wide, (h + 1) * wide)
            dk = dk_p[at, keyed] + to_end[at, keyed] * dot(
                values[at, valued], narrow[keyed, :], NT, None
            )
            dv = dv_p[at, valued] + dot(ke[at, keyed], narrow[keyed, :], NN, None)
            dk_v[at, keyed] = dk.astype(BF16)
            dv_v[at, valued] = dv.astype(BF16)
            moved = queries[at, keyed].astype(F32) * dq[at, keyed] - keys[at, keyed].astype(
                F32
            ) * dk
            dl_v[at, keyed] = dot(upper, moved, NN) + dot(ones, grown[keyed, :], NT)
        if n:
            g_end = mid[n] + fall[n] * g_end
    for src, dst in [(dk_v, dk_o), (dv_v, dv_o), (dl_v, dl_o)]:
        store(src, dst)
    proj_v[...] = dot(proj_in[...], all_s[...], TN, None)
    store(proj_v, proj_o)
    for copy in stores:
        copy.wait()


def size_of(scratch):
    return sum(math.prod(s) * jnp.dtype(d).itemsize for s, d in scratch)


def call(kernel, outs, ins, args, scratch=(), sems=(), ident=None, flops=2 * 10**8):
    semaphores = [pltpu.SemaphoreType.DMA((count,)) for count in sems]
    limit = size_of(scratch) + (4 << 20)
    return pl.pallas_call(
        kernel,
        out_shape=[m(s, d) for m, s, d in outs],
        in_specs=[pl.BlockSpec(memory_space=m) for m in ins],
        out_specs=[pl.BlockSpec(memory_space=m) for m, s, d in outs],
        scratch_shapes=[pltpu.VMEM(s, d) for s, d in scratch] + semaphores,
        cost_estimate=pl.CostEstimate(flops=flops, bytes_accessed=10**6, transcendentals=0),
        compiler_params=pltpu.CompilerParams(
            collective_id=ident, has_side_effects=ident is not None, vmem_limit_bytes=limit
        ),
    )(*[
        pltpu.with_memory_space_constraint(a, m) if m == pltpu.HBM else a
        for m, a in zip(ins, args)
    ])


def on_device(
    moe_input,
    cotangent,
    route_expert,
    route_weight,
    w_gate,
    w_up,
    w_down,
    out_proj,
    saved_out,
    queries,
    keys,
    values,
    log_decay,
    span_state,
):
    rows, width = moe_input.shape
    groups = lax.axis_size("sp")
    depth = lax.axis_size("tp") // 2
    units = w_gate.shape[2]
    tokens = groups * rows
    channels, wide = queries.shape[1], span_state.shape[2]
    lanes = values.shape[1]
    fast, slow = pltpu.VMEM, pltpu.HBM
    packet_rows = -(-(groups + 1) // 8) * 8
    reach = math.isqrt(groups) - 1
    links = 4 * reach + 2 * reach * reach

    def both(*counts):
        return [count for count in counts for _ in range(2)]

    spans = rows // SPAN
    heads = channels // DK
    made = call(
        functools.partial(expert_kernel, groups, depth),
        [
            (fast, w_gate.shape, BF16),
            (fast, w_up.shape, BF16),
            (fast, w_down.shape, BF16),
            (fast, (tokens, lanes), BF16),
            (fast, (tokens, width // groups), BF16),
            (fast, (channels, wide), F32),
            (fast, (spans, channels, wide), F32),
            (fast, (spans, channels, wide), F32),
            (fast, (spans, channels, wide), F32),
            (fast, (rows, channels), F32),
            (fast, (rows, channels), BF16),
            (fast, (rows, channels), F32),
            (fast, (rows, channels), F32),
            (fast, (rows, lanes), F32),
        ],
        [slow] * 14,
        (
            moe_input, cotangent, saved_out, route_expert.T, route_weight.T, log_decay,
            w_gate, w_up, w_down, out_proj, queries, keys, values, span_state,
        ),
        scratch=[
            ((rows, width), BF16),
            ((groups, packet_rows, rows), F32),
            (out_proj.shape, BF16),
            (queries.shape, BF16),
            (keys.shape, BF16),
            (values.shape, BF16),
            (span_state.shape, F32),
            ((groups, channels, wide), BF16),
            ((groups - 1, channels, wide), F32),
            ((rows, channels), F32),
            ((rows, channels), F32),
            ((rows, channels), BF16),
            ((rows, channels), BF16),
            ((heads, rows, rows), BF16),
            ((tokens, width), BF16),
            ((tokens, width), BF16),
            ((tokens, width), BF16),
            ((tokens, units), BF16),
            ((tokens, units), BF16),
            ((tokens, units), BF16),
            ((width, units), BF16),
            ((width, units), BF16),
            ((units, width), BF16),
            ((units, width), BF16),
            ((width, units), BF16),
            ((tokens, width // 2), BF16),
            ((2 * rows, width // 2), F32),
            ((groups, rows, width // 2), BF16),
            ((groups - 1, rows, width // 2), BF16),
            ((rows, width // 2), BF16),
            ((depth - 1, rows // depth, width // 2), BF16),
            ((2, rows), jnp.int32),
            ((2, rows), F32),
            (log_decay.shape, F32),
        ],
        sems=[14] + both(
            links, links, 2 * (groups - 1), groups, CUTS * (groups - 1), CUTS * (depth - 1),
            CUTS * (depth - 1), CUTS * depth, groups - 1, groups - 1, groups - 1,
        ),
        ident=1,
        flops=10**10,
    )
    small = [
        ((width // groups, lanes), F32),
        (queries.shape, BF16),
        (keys.shape, BF16),
        (values.shape, BF16),
        (log_decay.shape, F32),
    ]
    return call(
        last_kernel,
        [
            (slow, w_gate.shape, BF16),
            (slow, w_up.shape, BF16),
            (slow, w_down.shape, BF16),
            *((slow, s, d) for s, d in small),
        ],
        [fast] * 17,
        (*made, queries, keys, values),
        scratch=small,
        sems=[8],
    )


def solution(mesh):
    placed = (
        P("sp", None),
        P("sp", None),
        P("sp", None),
        P("sp", None),
        P("sp", None, "tp"),
        P("sp", None, "tp"),
        P("sp", "tp", None),
        P("tp", None),
        P("sp", "tp"),
        P("sp", "tp"),
        P("sp", "tp"),
        P("sp", "tp"),
        P("sp", "tp"),
        P("sp", "tp", None),
    )
    return jax.shard_map(
        on_device,
        mesh=mesh,
        in_specs=placed,
        out_specs=(
            P("sp", None, "tp"),
            P("sp", None, "tp"),
            P("sp", "tp", None),
            P("sp", "tp"),
            P("sp", "tp"),
            P("sp", "tp"),
            P("sp", "tp"),
            P("sp", "tp"),
        ),
        check_vma=False,
    )
```

```python
import functools
import math

import jax
import jax.numpy as jnp
from jax import lax
from jax.experimental import pallas as pl
from jax.experimental.pallas import tpu as pltpu
from jax.sharding import PartitionSpec as P

DK = 64
SPAN = 64
CUTS = 2

HIGH = lax.Precision.HIGHEST
F32 = jnp.float32
BF16 = jnp.bfloat16


def dot(a, b, dims, precision=HIGH):
    return lax.dot_general(
        a, b, ((dims[0], dims[1]), ((), ())), precision=precision, preferred_element_type=F32
    )


NN = ((1,), (0,))
NT = ((1,), (1,))
TN = ((0,), (0,))


def triangle(size, upper):
    row = lax.broadcasted_iota(jnp.int32, (size, size), 0)
    col = lax.broadcasted_iota(jnp.int32, (size, size), 1)
    return ((row <= col) if upper else (row >= col)).astype(F32)


def there(sp=None, tp=None):
    where = {}
    if sp is not None:
        where["sp"] = sp
    if tp is not None:
        where["tp"] = tp
    return where


def greet(partners):
    barrier = pltpu.get_barrier_semaphore()
    for partner in partners:
        pl.semaphore_signal(
            barrier, inc=1, device_id=partner, device_id_type=pl.DeviceIdType.MESH
        )
    pl.semaphore_wait(barrier, len(partners))


def send(src, dst, sems, slot, partner):
    copy = pltpu.make_async_remote_copy(
        src_ref=src,
        dst_ref=dst,
        send_sem=sems[0].at[slot],
        recv_sem=sems[1].at[slot],
        device_id=partner,
        device_id_type=pl.DeviceIdType.MESH,
    )
    copy.start()
    return copy


def expert_kernel(
    n, depth, moe, cot, saved, experts_h, shares_h, decay_h, gate_h, up_h, down_h,
    out_h, query_h, key_h, value_h, state_h,
    gate_o, up_o, down_o, all_s, proj_in, after, mid, fall, ends, to_end, ke, dq_o, dk_o, dv_o,
    grad_in, packet, out_proj, queries, keys, values, state, starts, factors,
    grow, shrink, qd, kd, scores,
    all_a, all_b, routed, hidden, d_gate, d_upper, gate_w, up_w,
    gate_t, up_t, down_t,
    slots, mine, got_t, got_p, sum_z, got_z, experts, shares, decay, local, *sems,
):
    me, lane = lax.axis_index("sp"), lax.axis_index("tp")
    core, z = lax.rem(lane, 2), lax.div(lane, 2)
    side = math.isqrt(n)
    y, x = lax.div(me, side), lax.rem(me, side)
    rows, width = moe.shape
    units = hidden.shape[1]
    channels = decay.shape[1]
    split = rows // 2
    wide = width // 2
    cuts = CUTS
    part = wide // cuts
    piece = rows // depth
    far, near, small, twin_s, plane_s, z_s, back_s, twin_b, slice_s, slice_t, begin = (
        sems[2 * i : 2 * i + 2] for i in range(11)
    )

    def ds(start, size):
        return pl.ds(pl.multiple_of(start, size), size)

    def place(dy, dx):
        return lax.rem(y + dy + side, side) * side + lax.rem(x + dx + side, side)

    def half(block):
        return ds(block * rows + core * split, split)

    def whole(block):
        return ds(block * rows, rows)

    started = []

    def go(*args):
        copy = send(*args)
        started.append(copy)
        return copy

    twin = there(tp=lane + 1 - 2 * core)
    peers = [there(sp=lax.rem(me + d, n)) for d in range(1, n)]
    along = [lax.rem(z + d, depth) for d in range(1, depth)]
    lanes = [there(tp=2 * far_z + core) for far_z in along]
    loads = [
        pltpu.make_async_copy(src, dst, local.at[i])
        for i, (src, dst) in enumerate([
            (moe, all_a.at[whole(me)]),
            (cot, all_b.at[whole(me)]),
            (gate_h.at[0], gate_w),
            (up_h.at[0], up_w),
            (down_h.at[0], down_o.at[0]),
            (saved, all_s.at[whole(me)]),
            (experts_h, experts),
            (shares_h, shares),
            (decay_h, decay),
            (query_h, queries),
            (key_h, keys),
            (value_h, values),
            (state_h, state),
            (out_h, out_proj),
        ])
    ]
    for load in loads[:2] + loads[6:9] + loads[2:6] + loads[9:]:
        load.start()
    greet(peers + lanes + [twin])
    loads[0].wait()
    loads[1].wait()
    offsets = range(1, side)
    reach = side - 1
    first = {}

    def spread(turn, on_x, on_y):
        for d in offsets:
            base, at = 2 * turn * reach + d - 1, half(me)
            first["x", turn, d] = go(
                on_x.at[at], on_x.at[at], far, base, there(sp=place(0, d))
            )
            first["y", turn, d] = go(
                on_y.at[at], on_y.at[at], far, base + reach, there(sp=place(d, 0))
            )

    spread(0, all_b, all_a)
    for load in loads[6:9]:
        load.wait()
    index = lax.broadcasted_iota(jnp.int32, (n, rows), 0)
    packet[me, 0:n, :] = jnp.where(index == experts[0:1, :], shares[0:1, :], 0.0) + jnp.where(
        index == experts[1:2, :], shares[1:2, :], 0.0
    )
    packet[me, n : n + 1, 0:channels] = jnp.sum(decay[...], axis=0, keepdims=True)
    notes = [
        go(packet.at[me], packet.at[me], small, d, peer) for d, peer in enumerate(peers)
    ]
    spread(1, all_a, all_b)
    eye = lax.broadcasted_iota(jnp.int32, (rows, rows), 0) == lax.broadcasted_iota(
        jnp.int32, (rows, rows), 1
    )
    tile = 256 if units % 256 == 0 else 128

    def relay(copy, full, block, slot):
        copy.wait_recv()
        at = half(block)
        return go(full.at[at], full.at[at], near, slot, twin)

    def turn_over(src, dst):
        columns = src.shape[1]
        strip = 256 if columns % 256 == 0 else 128

        def step(i, carry):
            at = ds(i * 256, 256)
            for j in range(0, columns, strip):
                dst[j : j + strip, at] = src[at, j : j + strip].T
            return carry

        lax.fori_loop(0, src.shape[0] // 256, step, 0)

    def rows_of(ref, blocks):
        parts = [ref[whole(block), :] for block in blocks]
        return parts[0] if len(parts) == 1 else jnp.concatenate(parts, axis=0)

    def expert(blocks):
        for block in blocks:
            at = whole(block)
            line = packet[block, pl.ds(me, 1), :]
            scale = jnp.sum(jnp.where(eye, line, 0.0), axis=1, keepdims=True)
            routed[at, :] = (all_b[at, :].astype(F32) * scale).astype(BF16)
        for start in range(0, units, tile):
            j = slice(start, start + tile)
            gate = dot(rows_of(all_a, blocks), gate_w[:, j], NN, None)
            upper = dot(rows_of(all_a, blocks), up_w[:, j], NN, None)
            d_hidden = dot(rows_of(routed, blocks), down_t[:, j], NN, None)
            sigmoid_gate = jax.nn.sigmoid(gate)
            active = gate * sigmoid_gate
            made = [
                (hidden, active * upper),
                (d_upper, d_hidden * active),
                (
                    d_gate,
                    d_hidden * upper * sigmoid_gate * (1.0 + gate * (1.0 - sigmoid_gate)),
                ),
            ]
            for ref, value in made:
                for i, block in enumerate(blocks):
                    ref[whole(block), j] = value[i * rows : (i + 1) * rows].astype(BF16)

    def back(blocks, which, h):
        for j in range(h * part, (h + 1) * part, 256):
            to = ds(which * wide + j, 256)
            value = dot(rows_of(d_gate, blocks), gate_t[:, to], NN, None) + dot(
                rows_of(d_upper, blocks), up_t[:, to], NN, None
            )
            yield slice(j, j + 256), value

    wide_v = values.shape[1]
    heads = channels // DK
    value_dim = wide_v // heads
    spans = rows // SPAN
    row = lax.broadcasted_iota(jnp.int32, (rows, rows), 0)
    col = lax.broadcasted_iota(jnp.int32, (rows, rows), 1)
    causal = (row >= col) & (lax.div(row, SPAN) == lax.div(col, SPAN))

    def keyed(h):
        return slice(h * DK, (h + 1) * DK)

    def valued(h):
        return slice(h * value_dim, (h + 1) * value_dim)

    def span(i):
        return slice(i * SPAN, (i + 1) * SPAN)

    def prepare():
        c = dot(causal.astype(F32), decay[...], NN)
        ones = jnp.ones((SPAN, value_dim), F32)
        grow[...] = jnp.exp(c)
        shrink[...] = jnp.exp(-c)
        for i in range(spans):
            at = span(i)
            last = c[(i + 1) * SPAN - 1 : (i + 1) * SPAN, :]
            to_end[at, :] = jnp.exp(last - c[at, :])
            fall[i] = jnp.exp(dot(decay[at, :], ones, TN))
        qd[...] = (queries[...].astype(F32) * grow[...]).astype(BF16)
        kd[...] = (keys[...].astype(F32) * shrink[...]).astype(BF16)
        ke[...] = (keys[...].astype(F32) * to_end[...]).astype(BF16)
        for h in range(heads):
            scores[h] = jnp.where(
                causal, dot(qd[:, keyed(h)], kd[:, keyed(h)], NT, None), 0.0
            ).astype(BF16)
            for i in range(spans):
                ends[i, keyed(h), :] = fall[i, keyed(h), :] * state[i, keyed(h), :] + dot(
                    ke[span(i), keyed(h)], values[span(i), valued(h)], TN, None
                )

    crossing = {}

    def emit(*steps):
        blocks = [place(dy, dx) for dy, dx in steps]
        marks = [(dy % side) * side + dx % side for dy, dx in steps]
        expert(blocks)
        swaps = {}
        for h in range(cuts):
            for cut, value in back(blocks, 1 - core, h):
                for i, block in enumerate(blocks):
                    slots[whole(block), cut] = value[i * rows : (i + 1) * rows].astype(BF16)
            cut = slice(h * part, (h + 1) * part)
            for block, slot in zip(blocks, marks):
                swaps[slot, h] = go(
                    slots.at[whole(block), cut], got_t.at[slot, :, cut], twin_s,
                    cuts * slot + h, twin,
                )
        for h in range(cuts):
            for cut, value in back(blocks, core, h):
                mine[0 : len(blocks) * rows, cut] = value
            cut = slice(h * part, (h + 1) * part)
            for i, (block, slot) in enumerate(zip(blocks, marks)):
                swaps[slot, h].wait_recv()
                got_t[slot, :, cut] = (
                    mine[i * rows : (i + 1) * rows, cut] + got_t[slot, :, cut].astype(F32)
                ).astype(BF16)
                if slot:
                    crossing[slot, h] = go(
                        got_t.at[slot, :, cut], got_p.at[slot - 1, :, cut], plane_s,
                        cuts * (slot - 1) + h, there(sp=block),
                    )

    for load in loads[9:]:
        load.wait()
    prepare()
    for load in loads[2:5]:
        load.wait()
    turn_over(down_o.at[0], down_t)
    turn_over(gate_w, gate_t)
    turn_over(up_w, up_t)
    second, passed = {}, {}
    flat = 4 * reach
    square = reach * reach
    for d in offsets:
        passed["y", 0, d] = relay(first["y", 0, d], all_a, place(-d, 0), reach + d - 1)
        at = half(place(-d, 0))
        for e in offsets:
            second[0, d, e] = go(
                all_a.at[at], all_a.at[at], far, flat + (d - 1) * reach + e - 1,
                there(sp=place(0, e)),
            )
        passed["x", 0, d] = relay(first["x", 0, d], all_b, place(0, -d), d - 1)
        at = half(place(0, -d))
        for e in offsets:
            second[1, e, d] = go(
                all_b.at[at], all_b.at[at], far, flat + square + (e - 1) * reach + d - 1,
                there(sp=place(e, 0)),
            )
    emit((0, 0))
    for d in offsets:
        passed["x", 1, d] = relay(first["x", 1, d], all_a, place(0, -d), 2 * reach + d - 1)
        passed["y", 1, d] = relay(first["y", 1, d], all_b, place(-d, 0), 3 * reach + d - 1)
    for note in notes:
        note.wait_recv()
    order = lax.broadcasted_iota(jnp.int32, (n, channels), 0)
    decays = jnp.concatenate([packet[q, n : n + 1, 0:channels] for q in range(n)], axis=0)
    for d in range(n - 1):
        source = lax.rem(me + n - 1 - d, n)
        between = jnp.where((order > me) & (order < source), decays, 0.0)
        factor = jnp.exp(dot(between, jnp.ones((n, value_dim), F32), TN))
        factors[d] = jnp.where(source > me, factor, 0.0)
    for d in offsets:
        for turn in range(2):
            passed["x", turn, d].wait_recv()
            passed["y", turn, d].wait_recv()
        emit((0, -d), (-d, 0))
    for d in offsets:
        for e in offsets:
            base = flat + (d - 1) * reach + e - 1
            pair = [
                relay(second[0, d, e], all_a, place(-d, -e), base),
                relay(second[1, d, e], all_b, place(-d, -e), base + square),
            ]
            for copy in pair:
                copy.wait_recv()
            emit((-d, -e))

    def gate_up(i, carry):
        at = ds(i * 256, 256)
        gate_o[0, at, :] = dot(all_a[:, at], d_gate[...], TN, None).astype(BF16)
        up_o[0, at, :] = dot(all_a[:, at], d_upper[...], TN, None).astype(BF16)
        return carry

    def down(i, carry):
        at = ds(i * tile, tile)
        turned = hidden[:, at].T
        for j in range(0, width, 512):
            to = slice(j, j + 512)
            down_o[0, at, to] = dot(turned, routed[:, to], NN, None).astype(BF16)
        return carry

    steps = width // 256
    turns = units // tile
    lax.fori_loop(0, steps, gate_up, 0)
    third, fourth, fifth = {}, {}, []
    for h in range(cuts):
        cut = slice(h * part, (h + 1) * part)
        total = got_t[0, :, cut].astype(F32)
        for slot in range(1, n):
            crossing[slot, h].wait_recv()
            total = total + got_p[slot - 1, :, cut].astype(F32)
        sum_z[:, cut] = total.astype(BF16)
        for d in range(depth - 1):
            third[h, d] = go(
                sum_z.at[ds(along[d] * piece, piece), cut], got_z.at[d, :, cut], z_s,
                h * (depth - 1) + d, lanes[d],
            )
    loads[5].wait()
    at = whole(me)
    shared = [
        go(all_s.at[at], all_s.at[at], small, n - 1 + d, peer)
        for d, peer in enumerate(peers)
    ]
    lax.fori_loop(0, turns // 2, down, 0)
    kept = ds(z * piece, piece)
    for h in range(cuts):
        cut = slice(h * part, (h + 1) * part)
        to = ds(core * wide + h * part, part)
        total = all_b[ds(me * rows + z * piece, piece), to].astype(F32)
        total = total + sum_z[kept, cut].astype(F32)
        for d in range(depth - 1):
            third[h, d].wait_recv()
            total = total + got_z[d, :, cut].astype(F32)
        grad_in[kept, to] = total.astype(BF16)
        for d in range(depth - 1):
            fourth[h, d] = go(
                grad_in.at[kept, to], grad_in.at[kept, to], back_s,
                h * (depth - 1) + d, lanes[d],
            )
        fifth.append(
            go(grad_in.at[kept, to], grad_in.at[kept, to], twin_b, h * depth, twin)
        )
    lax.fori_loop(turns // 2, turns, down, 0)
    slab = width // n
    owned = n // 2

    def slab_copy(goal, d, block):
        return pltpu.make_async_remote_copy(
            src_ref=grad_in.at[:, ds(goal * slab, slab)],
            dst_ref=proj_in.at[whole(block)],
            send_sem=slice_s[0].at[d - 1],
            recv_sem=slice_s[1].at[d - 1],
            device_id=there(sp=goal),
            device_id_type=pl.DeviceIdType.MESH,
        )

    def each_slab(h, act):
        for j in range(h * owned // cuts, (h + 1) * owned // cuts):
            goal = core * owned + j

            @pl.when(goal != me)
            def _():
                act(slab_copy(goal, lax.rem(goal - me + n, n), me))

    for h in range(cuts):
        to = ds(core * wide + h * part, part)
        for d in range(depth - 1):
            fourth[h, d].wait_recv()
            at = ds(lax.rem(z + depth - 1 - d, depth) * piece, piece)
            fifth.append(
                go(grad_in.at[at, to], grad_in.at[at, to], twin_b, h * depth + d + 1, twin)
            )
        each_slab(h, lambda copy: copy.start())
    for copy in fifth:
        copy.wait_recv()
    mix = dot(grad_in[...], out_proj[...], NT, None)
    g = mix.astype(BF16)
    scale = DK**-0.5
    for h in range(heads):
        carry = None
        for i in reversed(range(spans)):
            local_g = scale * dot(qd[span(i), keyed(h)], g[span(i), valued(h)], TN, None)
            mid[i, keyed(h), :] = local_g
            carry = local_g if carry is None else local_g + fall[i, keyed(h), :] * carry
        starts[me, keyed(h), :] = carry.astype(BF16)
    opened = [go(starts.at[me], starts.at[me], begin, d, peers[d]) for d in range(n - 1)]
    proj_in[whole(me), :] = grad_in[:, ds(me * slab, slab)]
    for h in range(heads):
        gh = g[:, valued(h)]
        gv = jnp.where(causal, dot(gh, values[:, valued(h)], NT, None), 0.0).astype(BF16)
        past = jnp.concatenate([
            dot(gh[span(i), :], state[i, keyed(h), :].astype(BF16), NT, None)
            for i in range(spans)
        ], axis=0)
        dq_o[:, keyed(h)] = scale * grow[:, keyed(h)] * (
            dot(gv, kd[:, keyed(h)], NN, None) + past
        )
        dk_o[:, keyed(h)] = scale * shrink[:, keyed(h)] * dot(gv, qd[:, keyed(h)], TN, None)
        dv_o[:, valued(h)] = scale * dot(scores[h], gh, TN, None)
    total = jnp.zeros((channels, value_dim), F32)
    for d in range(n - 1):
        opened[d].wait_recv()
        total = total + factors[d] * starts[lax.rem(me + n - 1 - d, n)].astype(F32)
    after[...] = total
    holder = lax.div(me, owned)

    def passing(d):
        at = whole(lax.rem(me + n - d, n))
        return pltpu.make_async_remote_copy(
            src_ref=proj_in.at[at],
            dst_ref=proj_in.at[at],
            send_sem=slice_t[0].at[d - 1],
            recv_sem=slice_t[1].at[d - 1],
            device_id=twin,
            device_id_type=pl.DeviceIdType.MESH,
        )

    @pl.when(core == holder)
    def _():
        for d in range(1, n):
            slab_copy(me, d, lax.rem(me + n - d, n)).wait_recv()
            passing(d).start()
        for d in range(1, n):
            passing(d).wait_send()

    @pl.when(core != holder)
    def _():
        for d in range(1, n):
            passing(d).wait_recv()

    for h in range(cuts):
        each_slab(h, lambda copy: copy.wait_send())
    for copy in shared:
        copy.wait_recv()
    for copy in started:
        copy.wait_send()


def last_kernel(
    gate, up, down, all_s, proj_in, after, mid, fall, ends, to_end, ke, dq, dk_p, dv_p,
    queries, keys, values,
    gate_o, up_o, down_o, proj_o, dq_o, dk_o, dv_o, dl_o,
    proj_v, dq_v, dk_v, dv_v, dl_v, sems,
):
    stores = []

    def store(src, dst):
        copy = pltpu.make_async_copy(src, dst, sems.at[len(stores)])
        copy.start()
        stores.append(copy)

    for src, dst in [(gate, gate_o), (up, up_o), (down, down_o)]:
        store(src, dst)
    dq_v[...] = dq[...].astype(BF16)
    store(dq_v, dq_o)
    rows, channels = queries.shape
    heads = channels // DK
    wide = values.shape[1] // heads
    ones = jnp.ones((SPAN, wide), F32)
    upper = triangle(SPAN, True)
    g_end = after[...]
    for n in reversed(range(rows // SPAN)):
        at = slice(n * SPAN, (n + 1) * SPAN)
        narrow = g_end.astype(BF16)
        grown = ends[n] * g_end
        for h in range(heads):
            keyed = slice(h * DK, (h + 1) * DK)
            valued = slice(h * wide, (h + 1) * wide)
            dk = dk_p[at, keyed] + to_end[at, keyed] * dot(
                values[at, valued], narrow[keyed, :], NT, None
            )
            dv = dv_p[at, valued] + dot(ke[at, keyed], narrow[keyed, :], NN, None)
            dk_v[at, keyed] = dk.astype(BF16)
            dv_v[at, valued] = dv.astype(BF16)
            moved = queries[at, keyed].astype(F32) * dq[at, keyed] - keys[at, keyed].astype(
                F32
            ) * dk
            dl_v[at, keyed] = dot(upper, moved, NN) + dot(ones, grown[keyed, :], NT)
        if n:
            g_end = mid[n] + fall[n] * g_end
    for src, dst in [(dk_v, dk_o), (dv_v, dv_o), (dl_v, dl_o)]:
        store(src, dst)
    proj_v[...] = dot(proj_in[...], all_s[...], TN, None)
    store(proj_v, proj_o)
    for copy in stores:
        copy.wait()


def size_of(scratch):
    return sum(math.prod(s) * jnp.dtype(d).itemsize for s, d in scratch)


def call(kernel, outs, ins, args, scratch=(), sems=(), ident=None, flops=2 * 10**8):
    semaphores = [pltpu.SemaphoreType.DMA((count,)) for count in sems]
    limit = size_of(scratch) + (4 << 20)
    return pl.pallas_call(
        kernel,
        out_shape=[m(s, d) for m, s, d in outs],
        in_specs=[pl.BlockSpec(memory_space=m) for m in ins],
        out_specs=[pl.BlockSpec(memory_space=m) for m, s, d in outs],
        scratch_shapes=[pltpu.VMEM(s, d) for s, d in scratch] + semaphores,
        cost_estimate=pl.CostEstimate(flops=flops, bytes_accessed=10**6, transcendentals=0),
        compiler_params=pltpu.CompilerParams(
            collective_id=ident, has_side_effects=ident is not None, vmem_limit_bytes=limit
        ),
    )(*[
        pltpu.with_memory_space_constraint(a, m) if m == pltpu.HBM else a
        for m, a in zip(ins, args)
    ])


def on_device(
    moe_input,
    cotangent,
    route_expert,
    route_weight,
    w_gate,
    w_up,
    w_down,
    out_proj,
    saved_out,
    queries,
    keys,
    values,
    log_decay,
    span_state,
):
    rows, width = moe_input.shape
    groups = lax.axis_size("sp")
    depth = lax.axis_size("tp") // 2
    units = w_gate.shape[2]
    tokens = groups * rows
    channels, wide = queries.shape[1], span_state.shape[2]
    lanes = values.shape[1]
    fast, slow = pltpu.VMEM, pltpu.HBM
    packet_rows = -(-(groups + 1) // 8) * 8
    reach = math.isqrt(groups) - 1
    links = 4 * reach + 2 * reach * reach

    def both(*counts):
        return [count for count in counts for _ in range(2)]

    spans = rows // SPAN
    heads = channels // DK
    made = call(
        functools.partial(expert_kernel, groups, depth),
        [
            (fast, w_gate.shape, BF16),
            (fast, w_up.shape, BF16),
            (fast, w_down.shape, BF16),
            (fast, (tokens, lanes), BF16),
            (fast, (tokens, width // groups), BF16),
            (fast, (channels, wide), F32),
            (fast, (spans, channels, wide), F32),
            (fast, (spans, channels, wide), F32),
            (fast, (spans, channels, wide), F32),
            (fast, (rows, channels), F32),
            (fast, (rows, channels), BF16),
            (fast, (rows, channels), F32),
            (fast, (rows, channels), F32),
            (fast, (rows, lanes), F32),
        ],
        [slow] * 14,
        (
            moe_input, cotangent, saved_out, route_expert.T, route_weight.T, log_decay,
            w_gate, w_up, w_down, out_proj, queries, keys, values, span_state,
        ),
        scratch=[
            ((rows, width), BF16),
            ((groups, packet_rows, rows), F32),
            (out_proj.shape, BF16),
            (queries.shape, BF16),
            (keys.shape, BF16),
            (values.shape, BF16),
            (span_state.shape, F32),
            ((groups, channels, wide), BF16),
            ((groups - 1, channels, wide), F32),
            ((rows, channels), F32),
            ((rows, channels), F32),
            ((rows, channels), BF16),
            ((rows, channels), BF16),
            ((heads, rows, rows), BF16),
            ((tokens, width), BF16),
            ((tokens, width), BF16),
            ((tokens, width), BF16),
            ((tokens, units), BF16),
            ((tokens, units), BF16),
            ((tokens, units), BF16),
            ((width, units), BF16),
            ((width, units), BF16),
            ((units, width), BF16),
            ((units, width), BF16),
            ((width, units), BF16),
            ((tokens, width // 2), BF16),
            ((2 * rows, width // 2), F32),
            ((groups, rows, width // 2), BF16),
            ((groups - 1, rows, width // 2), BF16),
            ((rows, width // 2), BF16),
            ((depth - 1, rows // depth, width // 2), BF16),
            ((2, rows), jnp.int32),
            ((2, rows), F32),
            (log_decay.shape, F32),
        ],
        sems=[14] + both(
            links, links, 2 * (groups - 1), CUTS * groups, CUTS * (groups - 1), CUTS * (depth - 1),
            CUTS * (depth - 1), CUTS * depth, groups - 1, groups - 1, groups - 1,
        ),
        ident=1,
        flops=10**10,
    )
    small = [
        ((width // groups, lanes), F32),
        (queries.shape, BF16),
        (keys.shape, BF16),
        (values.shape, BF16),
        (log_decay.shape, F32),
    ]
    return call(
        last_kernel,
        [
            (slow, w_gate.shape, BF16),
            (slow, w_up.shape, BF16),
            (slow, w_down.shape, BF16),
            *((slow, s, d) for s, d in small),
        ],
        [fast] * 17,
        (*made, queries, keys, values),
        scratch=small,
        sems=[8],
    )


def solution(mesh):
    placed = (
        P("sp", None),
        P("sp", None),
        P("sp", None),
        P("sp", None),
        P("sp", None, "tp"),
        P("sp", None, "tp"),
        P("sp", "tp", None),
        P("tp", None),
        P("sp", "tp"),
        P("sp", "tp"),
        P("sp", "tp"),
        P("sp", "tp"),
        P("sp", "tp"),
        P("sp", "tp", None),
    )
    return jax.shard_map(
        on_device,
        mesh=mesh,
        in_specs=placed,
        out_specs=(
            P("sp", None, "tp"),
            P("sp", None, "tp"),
            P("sp", "tp", None),
            P("sp", "tp"),
            P("sp", "tp"),
            P("sp", "tp"),
            P("sp", "tp"),
            P("sp", "tp"),
        ),
        check_vma=False,
    )
```

```python
import functools
import math

import jax
import jax.numpy as jnp
from jax import lax
from jax.experimental import pallas as pl
from jax.experimental.pallas import tpu as pltpu
from jax.sharding import PartitionSpec as P

DK = 64
SPAN = 64
CUTS = 2

HIGH = lax.Precision.HIGHEST
F32 = jnp.float32
BF16 = jnp.bfloat16


def dot(a, b, dims, precision=HIGH):
    return lax.dot_general(
        a, b, ((dims[0], dims[1]), ((), ())), precision=precision, preferred_element_type=F32
    )


NN = ((1,), (0,))
NT = ((1,), (1,))
TN = ((0,), (0,))


def triangle(size, upper):
    row = lax.broadcasted_iota(jnp.int32, (size, size), 0)
    col = lax.broadcasted_iota(jnp.int32, (size, size), 1)
    return ((row <= col) if upper else (row >= col)).astype(F32)


def there(sp=None, tp=None):
    where = {}
    if sp is not None:
        where["sp"] = sp
    if tp is not None:
        where["tp"] = tp
    return where


def greet(partners):
    barrier = pltpu.get_barrier_semaphore()
    for partner in partners:
        pl.semaphore_signal(
            barrier, inc=1, device_id=partner, device_id_type=pl.DeviceIdType.MESH
        )
    pl.semaphore_wait(barrier, len(partners))


def send(src, dst, sems, slot, partner):
    copy = pltpu.make_async_remote_copy(
        src_ref=src,
        dst_ref=dst,
        send_sem=sems[0].at[slot],
        recv_sem=sems[1].at[slot],
        device_id=partner,
        device_id_type=pl.DeviceIdType.MESH,
    )
    copy.start()
    return copy


def expert_kernel(
    n, depth, moe, cot, saved, experts_h, shares_h, decay_h, gate_h, up_h, down_h,
    out_h, query_h, key_h, value_h, state_h,
    gate_o, up_o, down_o, all_s, proj_in, after, mid, fall, ends, to_end, ke, dq_o, dk_o, dv_o,
    grad_in, packet, out_proj, queries, keys, values, state, starts, factors,
    grow, shrink, qd, kd, scores,
    all_a, all_b, routed, hidden, d_gate, d_upper, gate_w, up_w,
    gate_t, up_t, down_t,
    slots, mine, got_t, got_p, sum_z, got_z, experts, shares, decay, local, *sems,
):
    me, lane = lax.axis_index("sp"), lax.axis_index("tp")
    core, z = lax.rem(lane, 2), lax.div(lane, 2)
    side = math.isqrt(n)
    y, x = lax.div(me, side), lax.rem(me, side)
    rows, width = moe.shape
    units = hidden.shape[1]
    channels = decay.shape[1]
    split = rows // 2
    wide = width // 2
    cuts = CUTS
    part = wide // cuts
    piece = rows // depth
    far, near, small, twin_s, plane_s, z_s, back_s, twin_b, slice_s, slice_t, begin = (
        sems[2 * i : 2 * i + 2] for i in range(11)
    )

    def ds(start, size):
        return pl.ds(pl.multiple_of(start, size), size)

    def place(dy, dx):
        return lax.rem(y + dy + side, side) * side + lax.rem(x + dx + side, side)

    def half(block):
        return ds(block * rows + core * split, split)

    def whole(block):
        return ds(block * rows, rows)

    started = []

    def go(*args):
        copy = send(*args)
        started.append(copy)
        return copy

    twin = there(tp=lane + 1 - 2 * core)
    peers = [there(sp=lax.rem(me + d, n)) for d in range(1, n)]
    along = [lax.rem(z + d, depth) for d in range(1, depth)]
    lanes = [there(tp=2 * far_z + core) for far_z in along]
    loads = [
        pltpu.make_async_copy(src, dst, local.at[i])
        for i, (src, dst) in enumerate([
            (moe, all_a.at[whole(me)]),
            (cot, all_b.at[whole(me)]),
            (gate_h.at[0], gate_w),
            (up_h.at[0], up_w),
            (down_h.at[0], down_o.at[0]),
            (saved, all_s.at[whole(me)]),
            (experts_h, experts),
            (shares_h, shares),
            (decay_h, decay),
            (query_h, queries),
            (key_h, keys),
            (value_h, values),
            (state_h, state),
            (out_h, out_proj),
        ])
    ]
    for load in loads[:2] + loads[6:9] + loads[2:6] + loads[9:]:
        load.start()
    greet(peers + lanes + [twin])
    loads[0].wait()
    loads[1].wait()
    offsets = range(1, side)
    reach = side - 1
    first = {}

    def spread(turn, on_x, on_y):
        for d in offsets:
            base, at = 2 * turn * reach + d - 1, half(me)
            first["x", turn, d] = go(
                on_x.at[at], on_x.at[at], far, base, there(sp=place(0, d))
            )
            first["y", turn, d] = go(
                on_y.at[at], on_y.at[at], far, base + reach, there(sp=place(d, 0))
            )

    spread(0, all_b, all_a)
    for load in loads[6:9]:
        load.wait()
    index = lax.broadcasted_iota(jnp.int32, (n, rows), 0)
    packet[me, 0:n, :] = jnp.where(index == experts[0:1, :], shares[0:1, :], 0.0) + jnp.where(
        index == experts[1:2, :], shares[1:2, :], 0.0
    )
    packet[me, n : n + 1, 0:channels] = jnp.sum(decay[...], axis=0, keepdims=True)
    notes = [
        go(packet.at[me], packet.at[me], small, d, peer) for d, peer in enumerate(peers)
    ]
    spread(1, all_a, all_b)
    eye = lax.broadcasted_iota(jnp.int32, (rows, rows), 0) == lax.broadcasted_iota(
        jnp.int32, (rows, rows), 1
    )
    tile = 256 if units % 256 == 0 else 128

    def relay(copy, full, block, slot):
        copy.wait_recv()
        at = half(block)
        return go(full.at[at], full.at[at], near, slot, twin)

    def turn_over(src, dst):
        columns = src.shape[1]
        strip = 256 if columns % 256 == 0 else 128

        def step(i, carry):
            at = ds(i * 256, 256)
            for j in range(0, columns, strip):
                dst[j : j + strip, at] = src[at, j : j + strip].T
            return carry

        lax.fori_loop(0, src.shape[0] // 256, step, 0)

    def rows_of(ref, blocks):
        parts = [ref[whole(block), :] for block in blocks]
        return parts[0] if len(parts) == 1 else jnp.concatenate(parts, axis=0)

    def expert(blocks):
        for block in blocks:
            at = whole(block)
            line = packet[block, pl.ds(me, 1), :]
            scale = jnp.sum(jnp.where(eye, line, 0.0), axis=1, keepdims=True)
            routed[at, :] = (all_b[at, :].astype(F32) * scale).astype(BF16)
        for start in range(0, units, tile):
            j = slice(start, start + tile)
            gate = dot(rows_of(all_a, blocks), gate_w[:, j], NN, None)
            upper = dot(rows_of(all_a, blocks), up_w[:, j], NN, None)
            d_hidden = dot(rows_of(routed, blocks), down_t[:, j], NN, None)
            sigmoid_gate = jax.nn.sigmoid(gate)
            active = gate * sigmoid_gate
            made = [
                (hidden, active * upper),
                (d_upper, d_hidden * active),
                (
                    d_gate,
                    d_hidden * upper * sigmoid_gate * (1.0 + gate * (1.0 - sigmoid_gate)),
                ),
            ]
            for ref, value in made:
                for i, block in enumerate(blocks):
                    ref[whole(block), j] = value[i * rows : (i + 1) * rows].astype(BF16)

    def back(blocks, which, h):
        for j in range(h * part, (h + 1) * part, 256):
            to = ds(which * wide + j, 256)
            value = dot(rows_of(d_gate, blocks), gate_t[:, to], NN, None) + dot(
                rows_of(d_upper, blocks), up_t[:, to], NN, None
            )
            yield slice(j, j + 256), value

    wide_v = values.shape[1]
    heads = channels // DK
    value_dim = wide_v // heads
    spans = rows // SPAN
    row = lax.broadcasted_iota(jnp.int32, (rows, rows), 0)
    col = lax.broadcasted_iota(jnp.int32, (rows, rows), 1)
    causal = (row >= col) & (lax.div(row, SPAN) == lax.div(col, SPAN))

    def keyed(h):
        return slice(h * DK, (h + 1) * DK)

    def valued(h):
        return slice(h * value_dim, (h + 1) * value_dim)

    def span(i):
        return slice(i * SPAN, (i + 1) * SPAN)

    def prepare():
        c = dot(causal.astype(F32), decay[...], NN)
        ones = jnp.ones((SPAN, value_dim), F32)
        grow[...] = jnp.exp(c)
        shrink[...] = jnp.exp(-c)
        for i in range(spans):
            at = span(i)
            last = c[(i + 1) * SPAN - 1 : (i + 1) * SPAN, :]
            to_end[at, :] = jnp.exp(last - c[at, :])
            fall[i] = jnp.exp(dot(decay[at, :], ones, TN))
        qd[...] = (queries[...].astype(F32) * grow[...]).astype(BF16)
        kd[...] = (keys[...].astype(F32) * shrink[...]).astype(BF16)
        ke[...] = (keys[...].astype(F32) * to_end[...]).astype(BF16)
        for h in range(heads):
            scores[h] = jnp.where(
                causal, dot(qd[:, keyed(h)], kd[:, keyed(h)], NT, None), 0.0
            ).astype(BF16)
            for i in range(spans):
                ends[i, keyed(h), :] = fall[i, keyed(h), :] * state[i, keyed(h), :] + dot(
                    ke[span(i), keyed(h)], values[span(i), valued(h)], TN, None
                )

    crossing = {}

    def emit(*steps):
        blocks = [place(dy, dx) for dy, dx in steps]
        marks = [(dy % side) * side + dx % side for dy, dx in steps]
        expert(blocks)
        swaps = {}
        for h in range(cuts):
            for cut, value in back(blocks, 1 - core, h):
                for i, block in enumerate(blocks):
                    slots[whole(block), cut] = value[i * rows : (i + 1) * rows].astype(BF16)
            cut = slice(h * part, (h + 1) * part)
            for block, slot in zip(blocks, marks):
                swaps[slot, h] = go(
                    slots.at[whole(block), cut], got_t.at[slot, :, cut], twin_s,
                    cuts * slot + h, twin,
                )
        for h in range(cuts):
            for cut, value in back(blocks, core, h):
                mine[0 : len(blocks) * rows, cut] = value
            cut = slice(h * part, (h + 1) * part)
            for i, (block, slot) in enumerate(zip(blocks, marks)):
                swaps[slot, h].wait_recv()
                got_t[slot, :, cut] = (
                    mine[i * rows : (i + 1) * rows, cut] + got_t[slot, :, cut].astype(F32)
                ).astype(BF16)
                if slot:
                    crossing[slot, h] = go(
                        got_t.at[slot, :, cut], got_p.at[slot - 1, :, cut], plane_s,
                        cuts * (slot - 1) + h, there(sp=block),
                    )

    for load in loads[9:]:
        load.wait()
    prepare()
    for load in loads[2:5]:
        load.wait()
    turn_over(down_o.at[0], down_t)
    turn_over(gate_w, gate_t)
    turn_over(up_w, up_t)
    second, passed = {}, {}
    flat = 4 * reach
    square = reach * reach
    for d in offsets:
        passed["y", 0, d] = relay(first["y", 0, d], all_a, place(-d, 0), reach + d - 1)
        at = half(place(-d, 0))
        for e in offsets:
            second[0, d, e] = go(
                all_a.at[at], all_a.at[at], far, flat + (d - 1) * reach + e - 1,
                there(sp=place(0, e)),
            )
        passed["x", 0, d] = relay(first["x", 0, d], all_b, place(0, -d), d - 1)
        at = half(place(0, -d))
        for e in offsets:
            second[1, e, d] = go(
                all_b.at[at], all_b.at[at], far, flat + square + (e - 1) * reach + d - 1,
                there(sp=place(e, 0)),
            )
    emit((0, 0))
    for d in offsets:
        passed["x", 1, d] = relay(first["x", 1, d], all_a, place(0, -d), 2 * reach + d - 1)
        passed["y", 1, d] = relay(first["y", 1, d], all_b, place(-d, 0), 3 * reach + d - 1)
    for note in notes:
        note.wait_recv()
    order = lax.broadcasted_iota(jnp.int32, (n, channels), 0)
    decays = jnp.concatenate([packet[q, n : n + 1, 0:channels] for q in range(n)], axis=0)
    for d in range(n - 1):
        source = lax.rem(me + n - 1 - d, n)
        between = jnp.where((order > me) & (order < source), decays, 0.0)
        factor = jnp.exp(dot(between, jnp.ones((n, value_dim), F32), TN))
        factors[d] = jnp.where(source > me, factor, 0.0)
    for d in offsets:
        for turn in range(2):
            passed["x", turn, d].wait_recv()
            passed["y", turn, d].wait_recv()
        emit((0, -d), (-d, 0))
    for d in offsets:
        for e in offsets:
            base = flat + (d - 1) * reach + e - 1
            pair = [
                relay(second[0, d, e], all_a, place(-d, -e), base),
                relay(second[1, d, e], all_b, place(-d, -e), base + square),
            ]
            for copy in pair:
                copy.wait_recv()
            emit((-d, -e))

    def gate_up(i, carry):
        at = ds(i * 256, 256)
        gate_o[0, at, :] = dot(all_a[:, at], d_gate[...], TN, None).astype(BF16)
        up_o[0, at, :] = dot(all_a[:, at], d_upper[...], TN, None).astype(BF16)
        return carry

    def down(i, carry):
        at = ds(i * tile, tile)
        turned = hidden[:, at].T
        for j in range(0, width, 512):
            to = slice(j, j + 512)
            down_o[0, at, to] = dot(turned, routed[:, to], NN, None).astype(BF16)
        return carry

    steps = width // 256
    turns = units // tile
    lax.fori_loop(0, steps, gate_up, 0)
    third, fourth, fifth = {}, {}, []
    for h in range(cuts):
        cut = slice(h * part, (h + 1) * part)
        total = got_t[0, :, cut].astype(F32)
        for slot in range(1, n):
            crossing[slot, h].wait_recv()
            total = total + got_p[slot - 1, :, cut].astype(F32)
        sum_z[:, cut] = total.astype(BF16)
        for d in range(depth - 1):
            third[h, d] = go(
                sum_z.at[ds(along[d] * piece, piece), cut], got_z.at[d, :, cut], z_s,
                h * (depth - 1) + d, lanes[d],
            )
    loads[5].wait()
    at = whole(me)
    shared = [
        go(all_s.at[at], all_s.at[at], small, n - 1 + d, peer)
        for d, peer in enumerate(peers)
    ]
    lax.fori_loop(0, turns // 2, down, 0)
    kept = ds(z * piece, piece)
    for h in range(cuts):
        cut = slice(h * part, (h + 1) * part)
        to = ds(core * wide + h * part, part)
        total = all_b[ds(me * rows + z * piece, piece), to].astype(F32)
        total = total + sum_z[kept, cut].astype(F32)
        for d in range(depth - 1):
            third[h, d].wait_recv()
            total = total + got_z[d, :, cut].astype(F32)
        grad_in[kept, to] = total.astype(BF16)
        for d in range(depth - 1):
            fourth[h, d] = go(
                grad_in.at[kept, to], grad_in.at[kept, to], back_s,
                h * (depth - 1) + d, lanes[d],
            )
        fifth.append(
            go(grad_in.at[kept, to], grad_in.at[kept, to], twin_b, h * depth, twin)
        )
    lax.fori_loop(turns // 2, turns, down, 0)
    slab = width // n
    owned = n // 2

    def slab_copy(goal, d, block):
        return pltpu.make_async_remote_copy(
            src_ref=grad_in.at[:, ds(goal * slab, slab)],
            dst_ref=proj_in.at[whole(block)],
            send_sem=slice_s[0].at[d - 1],
            recv_sem=slice_s[1].at[d - 1],
            device_id=there(sp=goal),
            device_id_type=pl.DeviceIdType.MESH,
        )

    def each_slab(h, act):
        for j in range(h * owned // cuts, (h + 1) * owned // cuts):
            goal = core * owned + j

            @pl.when(goal != me)
            def _():
                act(slab_copy(goal, lax.rem(goal - me + n, n), me))

    for h in range(cuts):
        to = ds(core * wide + h * part, part)
        for d in range(depth - 1):
            fourth[h, d].wait_recv()
            at = ds(lax.rem(z + depth - 1 - d, depth) * piece, piece)
            fifth.append(
                go(grad_in.at[at, to], grad_in.at[at, to], twin_b, h * depth + d + 1, twin)
            )
        each_slab(h, lambda copy: copy.start())
    for copy in fifth:
        copy.wait_recv()
    mix = dot(grad_in[...], out_proj[...], NT, None)
    g = mix.astype(BF16)
    scale = DK**-0.5
    for h in range(heads):
        carry = None
        for i in reversed(range(spans)):
            local_g = scale * dot(qd[span(i), keyed(h)], g[span(i), valued(h)], TN, None)
            mid[i, keyed(h), :] = local_g
            carry = local_g if carry is None else local_g + fall[i, keyed(h), :] * carry
        starts[me, keyed(h), :] = carry.astype(BF16)
    opened = [go(starts.at[me], starts.at[me], begin, d, peers[d]) for d in range(n - 1)]
    proj_in[whole(me), :] = grad_in[:, ds(me * slab, slab)]
    for h in range(heads):
        gh = g[:, valued(h)]
        gv = jnp.where(causal, dot(gh, values[:, valued(h)], NT, None), 0.0).astype(BF16)
        past = jnp.concatenate([
            dot(gh[span(i), :], state[i, keyed(h), :].astype(BF16), NT, None)
            for i in range(spans)
        ], axis=0)
        dq_o[:, keyed(h)] = scale * grow[:, keyed(h)] * (
            dot(gv, kd[:, keyed(h)], NN, None) + past
        )
        dk_o[:, keyed(h)] = scale * shrink[:, keyed(h)] * dot(gv, qd[:, keyed(h)], TN, None)
        dv_o[:, valued(h)] = scale * dot(scores[h], gh, TN, None)
    total = jnp.zeros((channels, value_dim), F32)
    for d in range(n - 1):
        opened[d].wait_recv()
        total = total + factors[d] * starts[lax.rem(me + n - 1 - d, n)].astype(F32)
    after[...] = total
    holder = lax.div(me, owned)

    def passing(d):
        at = whole(lax.rem(me + n - d, n))
        return pltpu.make_async_remote_copy(
            src_ref=proj_in.at[at],
            dst_ref=proj_in.at[at],
            send_sem=slice_t[0].at[d - 1],
            recv_sem=slice_t[1].at[d - 1],
            device_id=twin,
            device_id_type=pl.DeviceIdType.MESH,
        )

    @pl.when(core == holder)
    def _():
        for d in range(1, n):
            slab_copy(me, d, lax.rem(me + n - d, n)).wait_recv()
            passing(d).start()
        for d in range(1, n):
            passing(d).wait_send()

    @pl.when(core != holder)
    def _():
        for d in range(1, n):
            passing(d).wait_recv()

    for h in range(cuts):
        each_slab(h, lambda copy: copy.wait_send())
    for copy in shared:
        copy.wait_recv()
    for copy in started:
        copy.wait_send()


def last_kernel(
    gate, up, down, all_s, proj_in, after, mid, fall, ends, to_end, ke, dq, dk_p, dv_p,
    queries, keys, values,
    gate_o, up_o, down_o, proj_o, dq_o, dk_o, dv_o, dl_o,
    proj_v, dq_v, dk_v, dv_v, dl_v, moved, sems,
):
    stores = []

    def store(src, dst):
        copy = pltpu.make_async_copy(src, dst, sems.at[len(stores)])
        copy.start()
        stores.append(copy)

    for src, dst in [(gate, gate_o), (up, up_o), (down, down_o)]:
        store(src, dst)
    dq_v[...] = dq[...].astype(BF16)
    store(dq_v, dq_o)
    proj_v[...] = dot(proj_in[...], all_s[...], TN, None)
    store(proj_v, proj_o)
    rows, channels = queries.shape
    heads = channels // DK
    wide = values.shape[1] // heads
    ones = jnp.ones((SPAN, wide), F32)
    row = lax.broadcasted_iota(jnp.int32, (rows, rows), 0)
    col = lax.broadcasted_iota(jnp.int32, (rows, rows), 1)
    upper = (row <= col) & (lax.div(row, SPAN) == lax.div(col, SPAN))
    g_end = after[...]
    for n in reversed(range(rows // SPAN)):
        at = slice(n * SPAN, (n + 1) * SPAN)
        narrow = g_end.astype(BF16)
        dl_v[at, :] = dot(ones, ends[n] * g_end, NT)
        for h in range(heads):
            keyed = slice(h * DK, (h + 1) * DK)
            valued = slice(h * wide, (h + 1) * wide)
            dk = dk_p[at, keyed] + to_end[at, keyed] * dot(
                values[at, valued], narrow[keyed, :], NT, None
            )
            dv = dv_p[at, valued] + dot(ke[at, keyed], narrow[keyed, :], NN, None)
            moved[at, keyed] = dk
            dk_v[at, keyed] = dk.astype(BF16)
            dv_v[at, valued] = dv.astype(BF16)
        if n:
            g_end = mid[n] + fall[n] * g_end
    store(dk_v, dk_o)
    store(dv_v, dv_o)
    change = queries[...].astype(F32) * dq[...] - keys[...].astype(F32) * moved[...]
    dl_v[...] = dl_v[...] + dot(upper.astype(F32), change, NN)
    store(dl_v, dl_o)
    for copy in stores:
        copy.wait()


def size_of(scratch):
    return sum(math.prod(s) * jnp.dtype(d).itemsize for s, d in scratch)


def call(kernel, outs, ins, args, scratch=(), sems=(), ident=None, flops=2 * 10**8):
    semaphores = [pltpu.SemaphoreType.DMA((count,)) for count in sems]
    limit = size_of(scratch) + (4 << 20)
    return pl.pallas_call(
        kernel,
        out_shape=[m(s, d) for m, s, d in outs],
        in_specs=[pl.BlockSpec(memory_space=m) for m in ins],
        out_specs=[pl.BlockSpec(memory_space=m) for m, s, d in outs],
        scratch_shapes=[pltpu.VMEM(s, d) for s, d in scratch] + semaphores,
        cost_estimate=pl.CostEstimate(flops=flops, bytes_accessed=10**6, transcendentals=0),
        compiler_params=pltpu.CompilerParams(
            collective_id=ident, has_side_effects=ident is not None, vmem_limit_bytes=limit
        ),
    )(*[
        pltpu.with_memory_space_constraint(a, m) if m == pltpu.HBM else a
        for m, a in zip(ins, args)
    ])


def on_device(
    moe_input,
    cotangent,
    route_expert,
    route_weight,
    w_gate,
    w_up,
    w_down,
    out_proj,
    saved_out,
    queries,
    keys,
    values,
    log_decay,
    span_state,
):
    rows, width = moe_input.shape
    groups = lax.axis_size("sp")
    depth = lax.axis_size("tp") // 2
    units = w_gate.shape[2]
    tokens = groups * rows
    channels, wide = queries.shape[1], span_state.shape[2]
    lanes = values.shape[1]
    fast, slow = pltpu.VMEM, pltpu.HBM
    packet_rows = -(-(groups + 1) // 8) * 8
    reach = math.isqrt(groups) - 1
    links = 4 * reach + 2 * reach * reach

    def both(*counts):
        return [count for count in counts for _ in range(2)]

    spans = rows // SPAN
    heads = channels // DK
    made = call(
        functools.partial(expert_kernel, groups, depth),
        [
            (fast, w_gate.shape, BF16),
            (fast, w_up.shape, BF16),
            (fast, w_down.shape, BF16),
            (fast, (tokens, lanes), BF16),
            (fast, (tokens, width // groups), BF16),
            (fast, (channels, wide), F32),
            (fast, (spans, channels, wide), F32),
            (fast, (spans, channels, wide), F32),
            (fast, (spans, channels, wide), F32),
            (fast, (rows, channels), F32),
            (fast, (rows, channels), BF16),
            (fast, (rows, channels), F32),
            (fast, (rows, channels), F32),
            (fast, (rows, lanes), F32),
        ],
        [slow] * 14,
        (
            moe_input, cotangent, saved_out, route_expert.T, route_weight.T, log_decay,
            w_gate, w_up, w_down, out_proj, queries, keys, values, span_state,
        ),
        scratch=[
            ((rows, width), BF16),
            ((groups, packet_rows, rows), F32),
            (out_proj.shape, BF16),
            (queries.shape, BF16),
            (keys.shape, BF16),
            (values.shape, BF16),
            (span_state.shape, F32),
            ((groups, channels, wide), BF16),
            ((groups - 1, channels, wide), F32),
            ((rows, channels), F32),
            ((rows, channels), F32),
            ((rows, channels), BF16),
            ((rows, channels), BF16),
            ((heads, rows, rows), BF16),
            ((tokens, width), BF16),
            ((tokens, width), BF16),
            ((tokens, width), BF16),
            ((tokens, units), BF16),
            ((tokens, units), BF16),
            ((tokens, units), BF16),
            ((width, units), BF16),
            ((width, units), BF16),
            ((units, width), BF16),
            ((units, width), BF16),
            ((width, units), BF16),
            ((tokens, width // 2), BF16),
            ((2 * rows, width // 2), F32),
            ((groups, rows, width // 2), BF16),
            ((groups - 1, rows, width // 2), BF16),
            ((rows, width // 2), BF16),
            ((depth - 1, rows // depth, width // 2), BF16),
            ((2, rows), jnp.int32),
            ((2, rows), F32),
            (log_decay.shape, F32),
        ],
        sems=[14] + both(
            links, links, 2 * (groups - 1), CUTS * groups, CUTS * (groups - 1), CUTS * (depth - 1),
            CUTS * (depth - 1), CUTS * depth, groups - 1, groups - 1, groups - 1,
        ),
        ident=1,
        flops=10**10,
    )
    small = [
        ((width // groups, lanes), F32),
        (queries.shape, BF16),
        (keys.shape, BF16),
        (values.shape, BF16),
        (log_decay.shape, F32),
    ]
    return call(
        last_kernel,
        [
            (slow, w_gate.shape, BF16),
            (slow, w_up.shape, BF16),
            (slow, w_down.shape, BF16),
            *((slow, s, d) for s, d in small),
        ],
        [fast] * 17,
        (*made, queries, keys, values),
        scratch=[*small, (log_decay.shape, F32)],
        sems=[8],
    )


def solution(mesh):
    placed = (
        P("sp", None),
        P("sp", None),
        P("sp", None),
        P("sp", None),
        P("sp", None, "tp"),
        P("sp", None, "tp"),
        P("sp", "tp", None),
        P("tp", None),
        P("sp", "tp"),
        P("sp", "tp"),
        P("sp", "tp"),
        P("sp", "tp"),
        P("sp", "tp"),
        P("sp", "tp", None),
    )
    return jax.shard_map(
        on_device,
        mesh=mesh,
        in_specs=placed,
        out_specs=(
            P("sp", None, "tp"),
            P("sp", None, "tp"),
            P("sp", "tp", None),
            P("sp", "tp"),
            P("sp", "tp"),
            P("sp", "tp"),
            P("sp", "tp"),
            P("sp", "tp"),
        ),
        check_vma=False,
    )
```
